32 devices in a mesh: tp: 4 (over y, x), dp: 8 (over z, core).
Axes of the slice: x: 2, y: 2, z: 4, core: 2. Of those that a mesh axis runs over, the one named last changes fastest.
Arguments:
- hidden_vectors: bfloat16 [48, 4096], P('tp', 'dp'), may hold values from -8 to 8
- live_spans: int32 [24], P('dp'), may hold values from 1 to 2, as said below
- entry_rescale: bfloat16 [2, 4096], P(None, 'dp'), may hold values from 0.099609375 to 1.8984375
- query_weights: bfloat16 [2, 4096, 2048], P(None, 'dp', 'tp'), may hold values from -0.09375 to 0.09375
- address_weights: bfloat16 [2, 4096, 2048], P(None, 'dp', 'tp'), may hold values from -0.09375 to 0.09375
- content_weights: bfloat16 [2, 4096, 2048], P(None, 'dp', 'tp'), may hold values from -0.09375 to 0.09375
- fade_weights: bfloat16 [2, 4096, 2048], P(None, 'dp', 'tp'), may hold values from -0.09375 to 0.09375
- learning_speed_weights: bfloat16 [2, 4096, 2048], P(None, 'dp', 'tp'), may hold values from -0.09375 to 0.09375
- exit_valve_weights: bfloat16 [2, 4096, 2048], P(None, 'dp', 'tp'), may hold values from -0.09375 to 0.09375
- feature_fade_ceiling: float32 [2, 2048], P(None, 'tp'), may hold values from 0.02 to 2
- subspace_rescale: float32 [2, 2048], P(None, 'tp'), may hold values from 0.1 to 1.9
- exit_weights: bfloat16 [2, 2048, 4096], P(None, 'tp', 'dp'), may hold values from -0.125 to 0.125
- memories: float32 [2, 24, 32, 64, 64], P(None, 'dp', 'tp'), may hold values from -6 to 6
- extra_log_fade: float32 [2, 48, 32], P(None, 'dp', 'tp'), may hold values from -0.7 to 0
Outputs:
- hidden_out: bfloat16 [48, 4096], P('tp', 'dp')
- new_states: float32 [2, 24, 32, 64, 64], P(None, 'dp', 'tp')
The draws below stay inside these ranges and needn't reach their ends.
Inputs may be any that keep to these rules, and one draw needn't show every extreme that they name: `live_spans`: live slots of each sequence; some sequence has 2.
All inputs are finite; a program needn't handle non-finite values.
Results may differ from the reference program's by a relative error of at most 0.0075.
Values may be sent and summed in bfloat16 or wider, within the bound.
A program may use at most 64 MiB of HBM per device.

```python
import math
import jax
import jax.numpy as jnp
from jax import lax

D = 4096
HEADS = 32
HD = 64
WIDTH = 2048
STEPS = 2
SEQS = 24
TOKENS = 48


def draw_hidden_vectors(key, part):
    values = jnp.clip(jax.random.normal(key, (TOKENS, D), jnp.float32), -4.0, 4.0)
    ramp = 0.4 * 5.0 ** (jnp.arange(D, dtype=jnp.float32) / D)
    return (values * ramp[None, :]).astype(jnp.bfloat16)


def draw_live_spans(key, part):
    picker = jax.random.randint(jax.random.fold_in(key, 1), (SEQS,), 0, 4)
    longer = jax.random.randint(jax.random.fold_in(key, 2), (SEQS,), 2, STEPS + 1)
    result = jnp.where(picker == 0, longer, 1)
    return result.at[0].set(STEPS).astype(jnp.int32)


def draw_extra_log_fade(key, part):
    picker = jax.random.randint(jax.random.fold_in(key, 3), (2, TOKENS, HEADS), 0, 8)
    depth = jax.random.uniform(jax.random.fold_in(key, 4), (2, TOKENS, HEADS), jnp.float32, -0.7, -0.2)
    return jnp.where(picker == 0, depth, 0.0).astype(jnp.float32)


def block_levels(rng, extent, split, low, largest):
    factor_of, own = 1.0, jax.random.fold_in(rng, 6)
    for axis_at, shards_of in split:
        heights = jnp.exp(jax.random.uniform(jax.random.fold_in(own, axis_at), (shards_of,), jnp.float32, low / len(split), largest / len(split)))
        factor_of = factor_of * jnp.repeat(heights, extent[axis_at] // shards_of).reshape([-1 if axis == axis_at else 1 for axis in range(len(extent))])
    return factor_of


def scatter_about(stream_key, dims, deviation, limit, split=(), kind=jnp.bfloat16):
    values = jax.random.normal(stream_key, dims, jnp.float32) * deviation
    if len(split) > 0:
        values = block_levels(stream_key, dims, split, -0.22, 0.18) * values
    return jnp.clip(values, min=-limit, max=limit).astype(kind)


def setup_inputs(seed: int = 0) -> dict:
    arg_keys = jax.random.split(jax.random.key(seed), 15)
    hidden_vectors = draw_hidden_vectors(jax.random.fold_in(arg_keys[14], 71), 0)
    live_spans = draw_live_spans(jax.random.fold_in(arg_keys[14], 71), 0)
    entry_rescale = jnp.clip(1.0 + 0.18 * jax.random.normal(arg_keys[2], (2, D), jnp.float32), 0.099609375, 1.8984375).astype(jnp.bfloat16)
    query_weights = scatter_about(arg_keys[3], (2, D, WIDTH), D ** -0.5, 0.09375, ((1, 8), (2, 4)))
    address_weights = scatter_about(arg_keys[4], (2, D, WIDTH), D ** -0.5, 0.09375, ((1, 8), (2, 4)))
    content_weights = scatter_about(arg_keys[5], (2, D, WIDTH), D ** -0.5, 0.09375, ((1, 8), (2, 4)))
    fade_weights = scatter_about(arg_keys[6], (2, D, WIDTH), D ** -0.5, 0.09375, ((1, 8), (2, 4)))
    learning_speed_weights = scatter_about(arg_keys[7], (2, D, WIDTH), D ** -0.5, 0.09375, ((1, 8), (2, 4)))
    exit_valve_weights = scatter_about(arg_keys[8], (2, D, WIDTH), D ** -0.5, 0.09375, ((1, 8), (2, 4)))
    feature_fade_ceiling = jnp.clip(jnp.exp(math.log(2.0) - 4.6051702 * jax.random.uniform(arg_keys[9], (2, WIDTH), jnp.float32) ** block_levels(arg_keys[9], (2, WIDTH), ((1, 4),), -0.2, 0.2)), 0.02, 2.0)
    subspace_rescale = jnp.clip(1.0 + 0.18 * jax.random.normal(arg_keys[10], (2, WIDTH), jnp.float32), 0.1, 1.9)
    exit_weights = scatter_about(arg_keys[11], (2, WIDTH, D), WIDTH ** -0.5, 0.125, ((1, 4), (2, 8)))
    memories = scatter_about(arg_keys[12], (2, SEQS, HEADS, HD, HD), 1.0, 6.0, ((1, 8), (2, 4)), jnp.float32)
    extra_log_fade = draw_extra_log_fade(jax.random.fold_in(arg_keys[14], 71), 0)
    return dict(hidden_vectors=hidden_vectors, live_spans=live_spans, entry_rescale=entry_rescale, query_weights=query_weights, address_weights=address_weights, content_weights=content_weights, fade_weights=fade_weights, learning_speed_weights=learning_speed_weights, exit_valve_weights=exit_valve_weights, feature_fade_ceiling=feature_fade_ceiling, subspace_rescale=subspace_rescale, exit_weights=exit_weights, memories=memories, extra_log_fade=extra_log_fade)


NORM_EPS = 1e-06
GROUP_EPS = 0.00064

def memory_change(mapped_vectors, live_spans, feature_fade_ceiling, subspace_rescale, running_memory, extra_log_fade):
    batch_total, subspace_total, subspace_size = (running_memory.shape[0], running_memory.shape[1], running_memory.shape[2])
    position_total = mapped_vectors[0].shape[0] // batch_total

    def by_head(values):
        return values.reshape(batch_total, position_total, subspace_total, subspace_size)
    read_rows, key_rows, value_rows, fade_scores, rate_pre, gate_pre = [by_head(v) for v in mapped_vectors]
    fade_multiplier_lines = jnp.exp(extra_log_fade.reshape(batch_total, position_total, subspace_total, 1) - feature_fade_ceiling.reshape(subspace_total, subspace_size) * jax.nn.sigmoid(fade_scores))
    rate_rows = jax.nn.sigmoid(rate_pre)
    gate_rows = jax.nn.sigmoid(gate_pre)
    unit_keys = key_rows * lax.rsqrt(lax.optimization_barrier(jnp.sum(key_rows * key_rows, axis=3, keepdims=True)) + 1e-06)
    readouts = []
    for position in range(position_total):
        is_live = (live_spans > position).reshape(batch_total, 1, 1, 1)
        unit_now = unit_keys[:, position]
        removed = jnp.einsum('shvk,shk->shv', running_memory, -unit_now, precision=lax.Precision.HIGHEST)
        updated = running_memory * fade_multiplier_lines[:, position][:, :, None, :] + removed[..., None] * (unit_now * rate_rows[:, position])[:, :, None, :] + value_rows[:, position][..., None] * key_rows[:, position][:, :, None, :]
        running_memory = jnp.where(is_live, updated, running_memory)
        readouts.append(jnp.einsum('shvk,shk->shv', running_memory, read_rows[:, position], precision=lax.Precision.HIGHEST))
    readout = jnp.stack(readouts, axis=1)
    centered = readout - lax.optimization_barrier(jnp.mean(readout, axis=3, keepdims=True))
    normed = centered * lax.rsqrt(lax.optimization_barrier(jnp.mean(centered * centered, axis=3, keepdims=True)) + GROUP_EPS)
    normed = normed * subspace_rescale.reshape(subspace_total, subspace_size)
    live_rows = (jnp.arange(position_total)[None, :] < live_spans[:, None]).astype(jnp.float32)[:, :, None, None]
    blended_result = (normed * gate_rows * live_rows).astype(jnp.bfloat16)
    return (blended_result.reshape(batch_total * position_total, subspace_total * subspace_size), running_memory)

def reference(hidden_vectors, live_spans, entry_rescale, query_weights, address_weights, content_weights, fade_weights, learning_speed_weights, exit_valve_weights, feature_fade_ceiling, subspace_rescale, exit_weights, memories, extra_log_fade):
    rows_now = hidden_vectors
    new_states = []
    for layer_ordinal in range(2):
        float_rows = rows_now.astype(jnp.float32)
        row_scale = lax.rsqrt(lax.optimization_barrier(jnp.mean(float_rows * float_rows, axis=1)) + NORM_EPS)[:, None]
        gained = (float_rows * entry_rescale[layer_ordinal].astype(jnp.float32)).astype(jnp.bfloat16)
        mapped_vectors = tuple((jnp.dot(gained, weights[layer_ordinal], preferred_element_type=jnp.float32) * row_scale for weights in (query_weights, address_weights, content_weights, fade_weights, learning_speed_weights, exit_valve_weights)))
        blended_result, running_memory = memory_change(mapped_vectors, live_spans, feature_fade_ceiling[layer_ordinal], subspace_rescale[layer_ordinal], memories[layer_ordinal], extra_log_fade[layer_ordinal])
        mix_rows = jnp.dot(blended_result, exit_weights[layer_ordinal], preferred_element_type=jnp.float32)
        rows_now = (float_rows + mix_rows).astype(jnp.bfloat16)
        new_states.append(running_memory)
    return (rows_now, jnp.stack(new_states))
```

```python
import functools

import jax
import jax.numpy as jnp
from jax import lax
from jax.experimental import pallas as pl
from jax.experimental.pallas import tpu as pltpu
from jax.sharding import PartitionSpec as P

NORM_EPS = 1e-06
KEY_EPS = 1e-06
GROUP_EPS = 0.00064
PAD = 8
EXTRA = 128
F32 = jnp.float32
BF16 = jnp.bfloat16


def kernel(
    n_tp,
    n_dp,
    x_hbm,
    live_ref,
    gain_hbm,
    w0,
    w1,
    w2,
    w3,
    w4,
    w5,
    ceiling_hbm,
    rescale_hbm,
    exit_hbm,
    memory_hbm,
    fade_hbm,
    out_ref,
    state_hbm,
    wv,
    ev,
    mem,
    gx,
    xs,
    ms,
    pown,
    dsend,
    drecv,
    zsend,
    zrecv,
    pr,
    mbuf,
    psend,
    precv,
    gain_ref,
    ceiling_ref,
    rescale_ref,
    fade_ref,
    s_high,
    s_low,
    load_sem,
    store_sem,
    send_sem,
    recv_sem,
):
    blocks = wv.shape[0]
    feats = x_hbm.shape[1]
    chans = wv.shape[3]
    seqs, heads, size = mem.shape[1], mem.shape[2], mem.shape[3]
    rows = zsend.shape[2]
    steps = rows // seqs
    half = 3 * chans
    nz = n_dp // 2
    per_tp = n_dp // n_tp

    tp = lax.axis_index("tp")
    dp = lax.axis_index("dp")
    z = dp // 2
    core = dp % 2
    other = 1 - core

    def peer(tp_at, dp_at):
        return {"tp": tp_at, "dp": dp_at}

    def tp_to(k):
        return lax.rem(tp + k, n_tp)

    def dp_to(dz, flip):
        return lax.rem(z + dz, nz) * 2 + (other if flip else core)

    def dp_from(dz, flip):
        return lax.rem(z + nz - dz, nz) * 2 + (other if flip else core)

    dp_offsets = [(dz, f) for dz in range(nz) for f in range(2) if (dz, f) != (0, 0)]
    far_first = sorted(dp_offsets, key=lambda o: -min(o[0], nz - o[0]))

    def slot_major(values):
        return jnp.concatenate(
            [
                values[s * steps + t : s * steps + t + 1]
                for t in range(steps)
                for s in range(seqs)
            ],
            axis=0,
        )

    def sequence_major(values):
        return jnp.concatenate(
            [
                values[t * seqs + s : t * seqs + s + 1]
                for s in range(seqs)
                for t in range(steps)
            ],
            axis=0,
        )

    counter = [0]

    def remote(src, dst, to):
        at = counter[0]
        counter[0] += 1
        return pltpu.make_async_remote_copy(
            src_ref=src,
            dst_ref=dst,
            send_sem=send_sem.at[at],
            recv_sem=recv_sem.at[at],
            device_id=to,
            device_id_type=pl.DeviceIdType.MESH,
        )

    weights = (w0, w1, w2, w3, w4, w5)
    loads = {}

    def load(name, src, dst):
        copy = pltpu.make_async_copy(src, dst, load_sem.at[len(loads)])
        copy.start()
        loads[name] = copy

    own_x = pltpu.make_async_copy(x_hbm, gx.at[tp], load_sem.at[load_sem.shape[0] - 1])
    own_x.start()
    load("gain", gain_hbm, gain_ref)
    load("ceiling", ceiling_hbm, ceiling_ref)
    load("rescale", rescale_hbm, rescale_ref)
    load("fade", fade_hbm, fade_ref)
    for b in range(blocks):
        for p in range(6):
            load(("w", b, p), weights[p].at[b], wv.at[b, p])
        load(("m", b), memory_hbm.at[b], mem.at[b])
        load(("e", b), exit_hbm.at[b], ev.at[b])

    barrier = pltpu.get_barrier_semaphore()
    for k in range(1, n_tp):
        pl.semaphore_signal(
            barrier, inc=1, device_id=peer(tp_to(k), dp), device_id_type=pl.DeviceIdType.MESH
        )
    for dz, f in dp_offsets:
        pl.semaphore_signal(
            barrier, inc=1, device_id=peer(tp, dp_to(dz, f)), device_id_type=pl.DeviceIdType.MESH
        )
    xs[...] = jnp.zeros_like(xs)
    ms[...] = jnp.zeros_like(ms)
    pr[...] = jnp.zeros_like(pr)
    own_x.wait()
    pl.semaphore_wait(barrier, n_tp - 1 + len(dp_offsets))

    outgoing = []

    first = []
    for k in range(1, n_tp):
        copy = remote(gx.at[tp], gx.at[tp], peer(tp_to(k), dp))
        copy.start()
        first.append(copy)
    for copy in first:
        copy.wait_recv()
    outgoing += first
    for i in range(n_tp):
        whole = gx[i].astype(F32)
        for g in range(per_tp):
            xs[(i * per_tp + g) * PAD : (i * per_tp + g) * PAD + rows, :] = slot_major(
                whole[g * rows : (g + 1) * rows]
            )
    for name in ("gain", "ceiling", "rescale", "fade"):
        loads[name].wait()

    row_at = lax.broadcasted_iota(jnp.int32, (PAD, 1), 0)
    live_col = jnp.zeros((PAD, 1), F32)
    for s in range(seqs):
        for t in range(steps):
            live_col = jnp.where(
                row_at == t * seqs + s, jnp.where(live_ref[s] > t, 1.0, 0.0), live_col
            )
    live3 = [
        live_col[t * seqs : (t + 1) * seqs].reshape(1, seqs, 1) for t in range(steps)
    ]
    extra_at = lax.broadcasted_iota(jnp.int32, (1, EXTRA), 1)

    for b in range(blocks):
        x_now = xs[...]
        gained = (x_now * gain_ref[b : b + 1, :].astype(F32)).astype(BF16)
        squares = jnp.sum(x_now * x_now, axis=1, keepdims=True)
        for p in range(6):
            loads[("w", b, p)].wait()

        high = squares.astype(BF16).astype(F32)
        split = jnp.where(extra_at < EXTRA // 2, high, squares - high)
        for j in range(n_dp):
            dsend[b, j, :, half : half + EXTRA] = split[j * PAD : j * PAD + rows].astype(BF16)
        piece = [pl.ds(p * chans, chans + (EXTRA if p == 2 else 0)) for p in range(3)]
        pairs = []
        for p in range(3):
            part = jnp.dot(gained, wv[b, 3 * other + p], preferred_element_type=F32)
            for j in range(n_dp):
                dsend[b, j, :, p * chans : (p + 1) * chans] = part[
                    j * PAD : j * PAD + rows
                ].astype(BF16)
            pair = remote(
                dsend.at[b, :, :, piece[p]], drecv.at[b, :, :, piece[p]], peer(tp, dp_to(0, 1))
            )
            pair.start()
            pairs.append(pair)
        outgoing += pairs
        ways = []
        for dz, f in far_first:
            to = dp_to(dz, f)
            copy = remote(zsend.at[b, to], zrecv.at[b, dz, core], peer(tp, to))
            at = counter[0] - 1
            arrives = pltpu.make_async_remote_copy(
                src_ref=zsend.at[b, to],
                dst_ref=zrecv.at[b, dz, other if f else core],
                send_sem=send_sem.at[at],
                recv_sem=recv_sem.at[at],
                device_id=peer(tp, to),
                device_id_type=pl.DeviceIdType.MESH,
            )
            ways.append((dz, to, at, copy, arrives))
        for p in range(3):
            own = jnp.dot(gained, wv[b, 3 * core + p], preferred_element_type=F32)
            pairs[p].wait_recv()
            for j in range(n_dp):
                zsend[b, j, :, p * chans : (p + 1) * chans] = (
                    own[j * PAD : j * PAD + rows]
                    + drecv[b, j, :, p * chans : (p + 1) * chans].astype(F32)
                ).astype(BF16)
                if p == 2:
                    given = drecv[b, j, :, half : half + EXTRA].astype(F32)
                    both = squares[j * PAD : j * PAD + rows] + jnp.sum(
                        given, axis=1, keepdims=True
                    ) * (2.0 / EXTRA)
                    both_high = both.astype(BF16).astype(F32)
                    zsend[b, j, :, half : half + EXTRA] = jnp.where(
                        extra_at < EXTRA // 2, both_high, both - both_high
                    ).astype(BF16)
            for dz, to, at, copy, arrives in ways:
                pltpu.make_async_remote_copy(
                    src_ref=zsend.at[b, to, :, piece[p]],
                    dst_ref=zrecv.at[b, dz, core, :, piece[p]],
                    send_sem=send_sem.at[at],
                    recv_sem=recv_sem.at[at],
                    device_id=peer(tp, to),
                    device_id_type=pl.DeviceIdType.MESH,
                ).start()
        scattered = [(copy, arrives) for dz, to, at, copy, arrives in ways]
        zrecv[b, 0, core] = zsend[b, dp]
        loads[("m", b)].wait()
        for s in range(seqs):
            state = mem[b, s].reshape(heads * size, size)
            state_high = state.astype(BF16)
            s_high[s] = state_high
            s_low[s] = (state - state_high.astype(F32)).astype(BF16)
        fade_b = slot_major(fade_ref[:, b, :])
        for copy, arrives in reversed(scattered):
            arrives.wait_recv()
            outgoing.append(copy)

        total_squares = jnp.zeros((rows, 1), F32)
        for dz in range(nz):
            total_squares = total_squares + jnp.sum(
                zrecv[b, dz, 0, :, half : half + EXTRA].astype(F32), axis=1, keepdims=True
            ) * (2.0 / EXTRA)
        row_scale = lax.rsqrt(total_squares / (feats * n_dp) + NORM_EPS)
        for h in range(2):
            total = zrecv[b, 0, h, :, 0:half].astype(F32)
            for dz in range(1, nz):
                total = total + zrecv[b, dz, h, :, 0:half].astype(F32)
            pr[0:rows, h * half : (h + 1) * half] = total * row_scale

        def by_head(p):
            values = pr[:, p * chans : (p + 1) * chans]
            return jnp.stack([values[:, h * size : (h + 1) * size] for h in range(heads)])

        read3, key3, value3 = by_head(0), by_head(1), by_head(2)
        fade3, rate3 = by_head(3), by_head(4)
        ceiling = ceiling_ref[b : b + 1, :]
        decay3 = []
        for h in range(heads):
            extra = jnp.concatenate(
                [fade_b[:, h : h + 1], jnp.zeros((PAD - rows, 1), F32)], axis=0
            )
            decay3.append(
                jnp.exp(
                    extra - ceiling[:, h * size : (h + 1) * size] * jax.nn.sigmoid(fade3[h])
                )
            )
        decay3 = jnp.stack(decay3)
        unit3 = key3 * lax.rsqrt(jnp.sum(key3 * key3, axis=2, keepdims=True) + KEY_EPS)
        pull3 = unit3 * jax.nn.sigmoid(rate3)

        def slots(values):
            return [values[:, t * seqs : (t + 1) * seqs, :] for t in range(steps)]

        read, key, value = slots(read3), slots(key3), slots(value3)
        decay, unit, pull = slots(decay3), slots(unit3), slots(pull3)

        wanted = []
        before = None
        for t in range(steps):
            wanted.append(unit[t] if before is None else before * unit[t])
            before = decay[t] if before is None else before * decay[t]
            wanted.append(before * read[t])
        kinds = len(wanted) * seqs
        deep = -(-kinds // 16) * 16
        wanted = jnp.concatenate(
            wanted + [jnp.zeros((heads, deep - kinds, size), F32)] * (deep > kinds), axis=1
        )
        wanted_high = wanted.astype(BF16).astype(F32)
        wanted_low = wanted - wanted_high
        together = max(d for d in range(1, heads + 1) if heads % d == 0 and d * size <= 256)
        found3 = []
        for first_head in range(0, heads, together):
            span = slice(first_head, first_head + together)
            lhs_high = wanted_high[span].reshape(together * deep, size).astype(BF16)
            lhs_low = wanted_low[span].reshape(together * deep, size).astype(BF16)
            found = None
            kind_at = lax.broadcasted_iota(jnp.int32, (together * deep, 1), 0) % deep % seqs
            for s in range(seqs):
                high_part = s_high[s, first_head * size : (first_head + together) * size, :]
                low_part = s_low[s, first_head * size : (first_head + together) * size, :]
                dims = (((1,), (1,)), ((), ()))
                product = (
                    lax.dot_general(lhs_high, high_part, dims, preferred_element_type=F32)
                    + lax.dot_general(lhs_low, high_part, dims, preferred_element_type=F32)
                    + lax.dot_general(lhs_high, low_part, dims, preferred_element_type=F32)
                )
                found = product if found is None else jnp.where(kind_at == s, product, found)
            for h in range(together):
                found3.append(found[h * deep : (h + 1) * deep, h * size : (h + 1) * size])
        found3 = jnp.stack(found3)
        base = [found3[:, i * seqs : (i + 1) * seqs, :] for i in range(2 * steps)]

        def dot3(a, c):
            return jnp.sum(a * c, axis=2, keepdims=True)

        taken = []

        def state_times(count, start, vector):
            total = start
            for i in range(count - 1, -1, -1):
                total = total - dot3(pull[i], vector) * taken[i] + dot3(key[i], vector) * value[i]
                if i:
                    vector = decay[i] * vector
            return total

        readouts = []
        for t in range(steps):
            taken.append(state_times(t, base[2 * t], unit[t]))
            readouts.append(state_times(t + 1, base[2 * t + 1], read[t]))
        readout = jnp.concatenate(readouts, axis=1)
        centered = readout - jnp.mean(readout, axis=2, keepdims=True)
        normed = centered * lax.rsqrt(
            jnp.mean(centered * centered, axis=2, keepdims=True) + GROUP_EPS
        )
        normed_rows = jnp.concatenate([normed[h] for h in range(heads)], axis=1)
        gate = jax.nn.sigmoid(pr[0:rows, 5 * chans : 6 * chans])
        mixed = normed_rows * rescale_ref[b : b + 1, :] * gate * live_col[0:rows]
        mbuf[b, dp] = mixed.astype(BF16)
        gathered = []
        for dz, f in far_first:
            to = dp_to(dz, f)
            copy = remote(mbuf.at[b, dp], mbuf.at[b, dp], peer(tp, to))
            copy.start()
            gathered.append(copy)

        left, right = [], []
        after = None
        for t in range(steps - 1, -1, -1):
            left += [-taken[t] * live3[t], value[t] * live3[t]]
            right += [pull[t] if after is None else pull[t] * after]
            right += [key[t] if after is None else key[t] * after]
            kept = jnp.where(live3[t] > 0.0, decay[t], 1.0)
            after = kept if after is None else after * kept
        filler = [jnp.zeros((heads, deep - kinds, size), F32)] * (deep > kinds)
        left = jnp.concatenate(left + filler, axis=1)
        right = jnp.concatenate(right + filler, axis=1)
        left_high = left.astype(BF16).astype(F32)
        right_high = right.astype(BF16).astype(F32)
        left = jnp.concatenate([left_high, left - left_high, left_high], axis=1).astype(BF16)
        right = jnp.concatenate([right_high, right_high, right - right_high], axis=1)
        slot_at = lax.broadcasted_iota(jnp.int32, (3 * deep, 1), 0) % deep % seqs
        for s in range(seqs):
            for h in range(heads):
                own = jnp.where(slot_at == s, right[h], 0.0).astype(BF16)
                state_hbm[b, s, h] = mem[b, s, h] * after[h, s : s + 1, :] + lax.dot_general(
                    left[h], own, (((0,), (0,)), ((), ())), preferred_element_type=F32
                )
        for copy in reversed(gathered):
            copy.wait_recv()
        outgoing += gathered
        for j in range(n_dp):
            ms[j * PAD : j * PAD + rows, :] = mbuf[b, j].astype(F32)
        loads[("e", b)].wait()
        part = jnp.dot(ms[...].astype(BF16), ev[b], preferred_element_type=F32)
        for j in range(n_dp):
            psend[b, j] = part[j * PAD : j * PAD + rows].astype(BF16)
        if b < blocks - 1:
            shared = []
            for k in range(1, n_tp):
                copy = remote(psend.at[b], precv.at[b, k - 1], peer(tp_to(k), dp))
                copy.start()
                shared.append(copy)
            for copy in shared:
                copy.wait_recv()
            outgoing += shared
            for j in range(n_dp):
                at = j * PAD
                total = part[at : at + rows]
                for k in range(1, n_tp):
                    total = total + precv[b, k - 1, j].astype(F32)
                xs[at : at + rows, :] = (x_now[at : at + rows] + total).astype(BF16).astype(F32)
        else:
            pown[:, 0:feats] = part
            shared = []
            for k in range(1, n_tp):
                copy = remote(
                    psend.at[b, pl.ds(tp_to(k) * per_tp, per_tp)],
                    precv.at[b, k - 1, pl.ds(0, per_tp)],
                    peer(tp_to(k), dp),
                )
                copy.start()
                shared.append(copy)
            for copy in shared:
                copy.wait_recv()
            outgoing += shared
            pieces = []
            for g in range(per_tp):
                at = pl.multiple_of((tp * per_tp + g) * PAD, PAD)
                total = pown[pl.ds(at, PAD), 0:feats][0:rows]
                for k in range(1, n_tp):
                    total = total + precv[b, k - 1, g].astype(F32)
                pieces.append(sequence_major(xs[pl.ds(at, PAD), :][0:rows] + total))
            out_ref[...] = jnp.concatenate(pieces, axis=0).astype(BF16)

    for copy in outgoing:
        copy.wait_send()


def store_kernel(out_vmem, state_vmem, out_hbm, state_hbm, sem):
    copies = [
        pltpu.make_async_copy(state_vmem, state_hbm, sem.at[0]),
        pltpu.make_async_copy(out_vmem, out_hbm, sem.at[1]),
    ]
    for copy in copies:
        copy.start()
    for copy in copies:
        copy.wait()


def solution(mesh):
    n_tp, n_dp = mesh.shape["tp"], mesh.shape["dp"]

    def shards(
        hidden,
        live,
        gain,
        w0,
        w1,
        w2,
        w3,
        w4,
        w5,
        ceiling,
        rescale,
        exit_w,
        memories,
        fade,
    ):
        blocks, feats, chans = w0.shape
        seqs, heads, size = memories.shape[1], memories.shape[2], memories.shape[3]
        rows = fade.shape[1]
        nz = n_dp // 2
        width = 3 * chans + EXTRA
        copies = (n_tp - 1) * (1 + blocks) + blocks * (3 + 2 * (n_dp - 1))
        vmem = pl.BlockSpec(memory_space=pltpu.VMEM)
        smem = pl.BlockSpec(memory_space=pltpu.SMEM)
        hbm = pl.BlockSpec(memory_space=pltpu.HBM)
        placed = pl.pallas_call(
            functools.partial(kernel, n_tp, n_dp),
            out_shape=(
                pltpu.VMEM(hidden.shape, hidden.dtype),
                pltpu.VMEM(memories.shape, memories.dtype),
            ),
            in_specs=[hbm, smem] + [hbm] * 12,
            out_specs=(vmem, vmem),
            scratch_shapes=[
                pltpu.VMEM((blocks, 6, feats, chans), BF16),
                pltpu.VMEM((blocks, chans, feats), BF16),
                pltpu.VMEM((blocks, seqs, heads, size, size), F32),
                pltpu.VMEM((n_tp,) + hidden.shape, BF16),
                pltpu.VMEM((n_dp * PAD, feats), F32),
                pltpu.VMEM((n_dp * PAD, chans), F32),
                pltpu.VMEM((n_dp * PAD, 3 * chans), F32),
                pltpu.VMEM((blocks, n_dp, rows, width), BF16),
                pltpu.VMEM((blocks, n_dp, rows, width), BF16),
                pltpu.VMEM((blocks, n_dp, rows, width), BF16),
                pltpu.VMEM((blocks, nz, 2, rows, width), BF16),
                pltpu.VMEM((PAD, 6 * chans), F32),
                pltpu.VMEM((blocks, n_dp, rows, chans), BF16),
                pltpu.VMEM((blocks, n_dp, rows, feats), BF16),
                pltpu.VMEM((blocks, n_tp - 1, n_dp, rows, feats), BF16),
                pltpu.VMEM(gain.shape, BF16),
                pltpu.VMEM(ceiling.shape, F32),
                pltpu.VMEM(rescale.shape, F32),
                pltpu.VMEM((rows, blocks, fade.shape[2]), F32),
                pltpu.VMEM((seqs, heads * size, size), BF16),
                pltpu.VMEM((seqs, heads * size, size), BF16),
                pltpu.SemaphoreType.DMA((blocks * 8 + 5,)),
                pltpu.SemaphoreType.DMA((blocks,)),
                pltpu.SemaphoreType.DMA((copies,)),
                pltpu.SemaphoreType.DMA((copies,)),
            ],
            compiler_params=pltpu.CompilerParams(
                collective_id=0, has_side_effects=True, vmem_limit_bytes=50000000
            ),
        )(hidden, live, gain, w0, w1, w2, w3, w4, w5, ceiling, rescale, exit_w, memories, fade.transpose(1, 0, 2))
        return pl.pallas_call(
            store_kernel,
            out_shape=(
                jax.ShapeDtypeStruct(hidden.shape, hidden.dtype),
                jax.ShapeDtypeStruct(memories.shape, memories.dtype),
            ),
            in_specs=[vmem, vmem],
            out_specs=(hbm, hbm),
            scratch_shapes=[pltpu.SemaphoreType.DMA((2,))],
            compiler_params=pltpu.CompilerParams(vmem_limit_bytes=1048576),
        )(*placed)

    in_specs = (
        P("tp", "dp"),
        P("dp"),
        P(None, "dp"),
        P(None, "dp", "tp"),
        P(None, "dp", "tp"),
        P(None, "dp", "tp"),
        P(None, "dp", "tp"),
        P(None, "dp", "tp"),
        P(None, "dp", "tp"),
        P(None, "tp"),
        P(None, "tp"),
        P(None, "tp", "dp"),
        P(None, "dp", "tp", None, None),
        P(None, "dp", "tp"),
    )
    out_specs = (P("tp", "dp"), P(None, "dp", "tp", None, None))
    return jax.shard_map(shards, mesh=mesh, in_specs=in_specs, out_specs=out_specs, check_vma=False)
```

```python
import functools

import jax
import jax.numpy as jnp
from jax import lax
from jax.experimental import pallas as pl
from jax.experimental.pallas import tpu as pltpu
from jax.sharding import PartitionSpec as P

NORM_EPS = 1e-06
KEY_EPS = 1e-06
GROUP_EPS = 0.00064
PAD = 8
LANES = 128
VMEM_BYTES = 67043328
EXTRA = 128
F32 = jnp.float32
BF16 = jnp.bfloat16


def kernel(
    n_tp,
    n_dp,
    x_hbm,
    live_ref,
    gain_hbm,
    w0,
    w1,
    w2,
    w3,
    w4,
    w5,
    ceiling_hbm,
    rescale_hbm,
    exit_hbm,
    memory_hbm,
    fade_hbm,
    out_ref,
    state_hbm,
    wv,
    ev,
    mem,
    gx,
    xs,
    ms,
    pown,
    dsend,
    drecv,
    zsend,
    zrecv,
    pr,
    mbuf,
    psend,
    precv,
    gain_ref,
    ceiling_ref,
    rescale_ref,
    fade_ref,
    s_high,
    s_low,
    load_sem,
    store_sem,
    send_sem,
    recv_sem,
):
    blocks = wv.shape[0]
    feats = x_hbm.shape[1]
    chans = wv.shape[3]
    seqs, heads, size = mem.shape[1], mem.shape[2], mem.shape[3]
    rows = zsend.shape[2]
    steps = rows // seqs
    half = 3 * chans
    nz = n_dp // 2
    per_tp = n_dp // n_tp

    tp = lax.axis_index("tp")
    dp = lax.axis_index("dp")
    z = dp // 2
    core = dp % 2
    other = 1 - core

    def peer(tp_at, dp_at):
        return {"tp": tp_at, "dp": dp_at}

    def tp_to(k):
        return lax.rem(tp + k, n_tp)

    def dp_to(dz, flip):
        return lax.rem(z + dz, nz) * 2 + (other if flip else core)

    def dp_from(dz, flip):
        return lax.rem(z + nz - dz, nz) * 2 + (other if flip else core)

    dp_offsets = [(dz, f) for dz in range(nz) for f in range(2) if (dz, f) != (0, 0)]
    far_first = sorted(dp_offsets, key=lambda o: -min(o[0], nz - o[0]))

    def slot_major(values):
        return jnp.concatenate(
            [
                values[s * steps + t : s * steps + t + 1]
                for t in range(steps)
                for s in range(seqs)
            ],
            axis=0,
        )

    def sequence_major(values):
        return jnp.concatenate(
            [
                values[t * seqs + s : t * seqs + s + 1]
                for s in range(seqs)
                for t in range(steps)
            ],
            axis=0,
        )

    counter = [0]

    def remote(src, dst, to):
        at = counter[0]
        counter[0] += 1
        return pltpu.make_async_remote_copy(
            src_ref=src,
            dst_ref=dst,
            send_sem=send_sem.at[at],
            recv_sem=recv_sem.at[at],
            device_id=to,
            device_id_type=pl.DeviceIdType.MESH,
        )

    weights = (w0, w1, w2, w3, w4, w5)
    loads = {}

    def load(name, src, dst):
        copy = pltpu.make_async_copy(src, dst, load_sem.at[len(loads)])
        copy.start()
        loads[name] = copy

    own_x = pltpu.make_async_copy(x_hbm, gx.at[tp], load_sem.at[load_sem.shape[0] - 1])
    own_x.start()
    load("gain", gain_hbm, gain_ref)
    load("ceiling", ceiling_hbm, ceiling_ref)
    load("rescale", rescale_hbm, rescale_ref)
    load("fade", fade_hbm, fade_ref)
    for b in range(blocks):
        for p in range(6):
            load(("w", b, p), weights[p].at[b], wv.at[b, p])
        load(("m", b), memory_hbm.at[b], mem.at[b])
        load(("e", b), exit_hbm.at[b], ev.at[b])

    barrier = pltpu.get_barrier_semaphore()
    for k in range(1, n_tp):
        pl.semaphore_signal(
            barrier, inc=1, device_id=peer(tp_to(k), dp), device_id_type=pl.DeviceIdType.MESH
        )
    for dz, f in dp_offsets:
        pl.semaphore_signal(
            barrier, inc=1, device_id=peer(tp, dp_to(dz, f)), device_id_type=pl.DeviceIdType.MESH
        )
    xs[...] = jnp.zeros_like(xs)
    ms[...] = jnp.zeros_like(ms)
    pr[...] = jnp.zeros_like(pr)
    own_x.wait()
    pl.semaphore_wait(barrier, n_tp - 1 + len(dp_offsets))

    outgoing = []

    first = []
    for k in range(1, n_tp):
        copy = remote(gx.at[tp], gx.at[tp], peer(tp_to(k), dp))
        copy.start()
        first.append(copy)
    for copy in first:
        copy.wait_recv()
    outgoing += first
    for i in range(n_tp):
        whole = gx[i].astype(F32)
        for g in range(per_tp):
            xs[(i * per_tp + g) * PAD : (i * per_tp + g) * PAD + rows, :] = slot_major(
                whole[g * rows : (g + 1) * rows]
            )
    for name in ("gain", "ceiling", "rescale", "fade"):
        loads[name].wait()

    row_at = lax.broadcasted_iota(jnp.int32, (PAD, 1), 0)
    live_col = jnp.zeros((PAD, 1), F32)
    for s in range(seqs):
        for t in range(steps):
            live_col = jnp.where(
                row_at == t * seqs + s, jnp.where(live_ref[s] > t, 1.0, 0.0), live_col
            )
    live3 = [
        live_col[t * seqs : (t + 1) * seqs].reshape(1, seqs, 1) for t in range(steps)
    ]
    extra_at = lax.broadcasted_iota(jnp.int32, (1, EXTRA), 1)

    for b in range(blocks):
        x_now = xs[...]
        gained = (x_now * gain_ref[b : b + 1, :].astype(F32)).astype(BF16)
        squares = jnp.sum(x_now * x_now, axis=1, keepdims=True)
        for p in range(6):
            loads[("w", b, p)].wait()

        high = squares.astype(BF16).astype(F32)
        split = jnp.where(extra_at < EXTRA // 2, high, squares - high)
        for j in range(n_dp):
            dsend[b, j, :, half : half + EXTRA] = split[j * PAD : j * PAD + rows].astype(BF16)
        piece = [pl.ds(p * chans, chans + (EXTRA if p == 2 else 0)) for p in range(3)]
        pairs = []
        for p in range(3):
            part = jnp.dot(gained, wv[b, 3 * other + p], preferred_element_type=F32)
            for j in range(n_dp):
                dsend[b, j, :, p * chans : (p + 1) * chans] = part[
                    j * PAD : j * PAD + rows
                ].astype(BF16)
            pair = remote(
                dsend.at[b, :, :, piece[p]], drecv.at[b, :, :, piece[p]], peer(tp, dp_to(0, 1))
            )
            pair.start()
            pairs.append(pair)
        outgoing += pairs
        ways = []
        for dz, f in far_first:
            to = dp_to(dz, f)
            copy = remote(zsend.at[b, to], zrecv.at[b, dz, core], peer(tp, to))
            at = counter[0] - 1
            arrives = pltpu.make_async_remote_copy(
                src_ref=zsend.at[b, to],
                dst_ref=zrecv.at[b, dz, other if f else core],
                send_sem=send_sem.at[at],
                recv_sem=recv_sem.at[at],
                device_id=peer(tp, to),
                device_id_type=pl.DeviceIdType.MESH,
            )
            ways.append((dz, to, at, copy, arrives))
        for p in range(3):
            own = jnp.dot(gained, wv[b, 3 * core + p], preferred_element_type=F32)
            pairs[p].wait_recv()
            for j in range(n_dp):
                zsend[b, j, :, p * chans : (p + 1) * chans] = (
                    own[j * PAD : j * PAD + rows]
                    + drecv[b, j, :, p * chans : (p + 1) * chans].astype(F32)
                ).astype(BF16)
                if p == 2:
                    given = drecv[b, j, :, half : half + EXTRA].astype(F32)
                    both = squares[j * PAD : j * PAD + rows] + jnp.sum(
                        given, axis=1, keepdims=True
                    ) * (2.0 / EXTRA)
                    both_high = both.astype(BF16).astype(F32)
                    zsend[b, j, :, half : half + EXTRA] = jnp.where(
                        extra_at < EXTRA // 2, both_high, both - both_high
                    ).astype(BF16)
            for dz, to, at, copy, arrives in ways:
                pltpu.make_async_remote_copy(
                    src_ref=zsend.at[b, to, :, piece[p]],
                    dst_ref=zrecv.at[b, dz, core, :, piece[p]],
                    send_sem=send_sem.at[at],
                    recv_sem=recv_sem.at[at],
                    device_id=peer(tp, to),
                    device_id_type=pl.DeviceIdType.MESH,
                ).start()
        scattered = [(copy, arrives) for dz, to, at, copy, arrives in ways]
        zrecv[b, 0, core] = zsend[b, dp]
        loads[("m", b)].wait()
        for s in range(seqs):
            state = mem[b, s].reshape(heads * size, size)
            state_high = state.astype(BF16)
            s_high[s] = state_high
            s_low[s] = (state - state_high.astype(F32)).astype(BF16)
        fade_b = slot_major(fade_ref[:, b, :])
        for copy, arrives in reversed(scattered):
            arrives.wait_recv()
            outgoing.append(copy)

        total_squares = jnp.zeros((rows, 1), F32)
        for dz in range(nz):
            total_squares = total_squares + jnp.sum(
                zrecv[b, dz, 0, :, half : half + EXTRA].astype(F32), axis=1, keepdims=True
            ) * (2.0 / EXTRA)
        row_scale = lax.rsqrt(total_squares / (feats * n_dp) + NORM_EPS)
        for h in range(2):
            total = zrecv[b, 0, h, :, 0:half].astype(F32)
            for dz in range(1, nz):
                total = total + zrecv[b, dz, h, :, 0:half].astype(F32)
            pr[0:rows, h * half : (h + 1) * half] = total * row_scale

        def by_head(p):
            values = pr[:, p * chans : (p + 1) * chans]
            return jnp.stack([values[:, h * size : (h + 1) * size] for h in range(heads)])

        read3, key3, value3 = by_head(0), by_head(1), by_head(2)
        fade3, rate3 = by_head(3), by_head(4)
        ceiling = ceiling_ref[b : b + 1, :]
        decay3 = []
        for h in range(heads):
            extra = jnp.concatenate(
                [fade_b[:, h : h + 1], jnp.zeros((PAD - rows, 1), F32)], axis=0
            )
            decay3.append(
                jnp.exp(
                    extra - ceiling[:, h * size : (h + 1) * size] * jax.nn.sigmoid(fade3[h])
                )
            )
        decay3 = jnp.stack(decay3)
        unit3 = key3 * lax.rsqrt(jnp.sum(key3 * key3, axis=2, keepdims=True) + KEY_EPS)
        pull3 = unit3 * jax.nn.sigmoid(rate3)

        def slots(values):
            return [values[:, t * seqs : (t + 1) * seqs, :] for t in range(steps)]

        read, key, value = slots(read3), slots(key3), slots(value3)
        decay, unit, pull = slots(decay3), slots(unit3), slots(pull3)

        wanted = []
        before = None
        for t in range(steps):
            wanted.append(unit[t] if before is None else before * unit[t])
            before = decay[t] if before is None else before * decay[t]
            wanted.append(before * read[t])
        kinds = len(wanted) * seqs
        deep = -(-kinds // 16) * 16
        wanted = jnp.concatenate(
            wanted + [jnp.zeros((heads, deep - kinds, size), F32)] * (deep > kinds), axis=1
        )
        wanted_high = wanted.astype(BF16).astype(F32)
        wanted_low = wanted - wanted_high
        together = max(d for d in range(1, heads + 1) if heads % d == 0 and d * size <= 256)
        found3 = []
        for first_head in range(0, heads, together):
            span = slice(first_head, first_head + together)
            lhs_high = wanted_high[span].reshape(together * deep, size).astype(BF16)
            lhs_low = wanted_low[span].reshape(together * deep, size).astype(BF16)
            found = None
            kind_at = lax.broadcasted_iota(jnp.int32, (together * deep, 1), 0) % deep % seqs
            for s in range(seqs):
                high_part = s_high[s, first_head * size : (first_head + together) * size, :]
                low_part = s_low[s, first_head * size : (first_head + together) * size, :]
                dims = (((1,), (1,)), ((), ()))
                product = (
                    lax.dot_general(lhs_high, high_part, dims, preferred_element_type=F32)
                    + lax.dot_general(lhs_low, high_part, dims, preferred_element_type=F32)
                    + lax.dot_general(lhs_high, low_part, dims, preferred_element_type=F32)
                )
                found = product if found is None else jnp.where(kind_at == s, product, found)
            for h in range(together):
                found3.append(found[h * deep : (h + 1) * deep, h * size : (h + 1) * size])
        found3 = jnp.stack(found3)
        base = [found3[:, i * seqs : (i + 1) * seqs, :] for i in range(2 * steps)]

        def dot3(a, c):
            return jnp.sum(a * c, axis=2, keepdims=True)

        taken = []

        def state_times(count, start, vector):
            total = start
            for i in range(count - 1, -1, -1):
                total = total - dot3(pull[i], vector) * taken[i] + dot3(key[i], vector) * value[i]
                if i:
                    vector = decay[i] * vector
            return total

        readouts = []
        for t in range(steps):
            taken.append(state_times(t, base[2 * t], unit[t]))
            readouts.append(state_times(t + 1, base[2 * t + 1], read[t]))
        readout = jnp.concatenate(readouts, axis=1)
        centered = readout - jnp.mean(readout, axis=2, keepdims=True)
        normed = centered * lax.rsqrt(
            jnp.mean(centered * centered, axis=2, keepdims=True) + GROUP_EPS
        )
        normed_rows = jnp.concatenate([normed[h] for h in range(heads)], axis=1)
        gate = jax.nn.sigmoid(pr[0:rows, 5 * chans : 6 * chans])
        mixed = normed_rows * rescale_ref[b : b + 1, :] * gate * live_col[0:rows]
        mbuf[b, dp] = mixed.astype(BF16)
        gathered = []
        for dz, f in far_first:
            to = dp_to(dz, f)
            copy = remote(mbuf.at[b, dp], mbuf.at[b, dp], peer(tp, to))
            copy.start()
            gathered.append(copy)

        left, right = [], []
        after = None
        for t in range(steps - 1, -1, -1):
            left += [-taken[t] * live3[t], value[t] * live3[t]]
            right += [pull[t] if after is None else pull[t] * after]
            right += [key[t] if after is None else key[t] * after]
            kept = jnp.where(live3[t] > 0.0, decay[t], 1.0)
            after = kept if after is None else after * kept
        filler = [jnp.zeros((heads, deep - kinds, size), F32)] * (deep > kinds)
        left = jnp.concatenate(left + filler, axis=1)
        right = jnp.concatenate(right + filler, axis=1)
        left_high = left.astype(BF16).astype(F32)
        right_high = right.astype(BF16).astype(F32)
        left = jnp.concatenate([left_high, left - left_high, left_high], axis=1).astype(BF16)
        right = jnp.concatenate([right_high, right_high, right - right_high], axis=1)
        slot_at = lax.broadcasted_iota(jnp.int32, (3 * deep, 1), 0) % deep % seqs
        for s in range(seqs):
            for h in range(heads):
                own = jnp.where(slot_at == s, right[h], 0.0).astype(BF16)
                state_hbm[b, s, h] = mem[b, s, h] * after[h, s : s + 1, :] + lax.dot_general(
                    left[h], own, (((0,), (0,)), ((), ())), preferred_element_type=F32
                )
        for copy in reversed(gathered):
            copy.wait_recv()
        outgoing += gathered
        for j in range(n_dp):
            ms[j * PAD : j * PAD + rows, :] = mbuf[b, j].astype(F32)
        loads[("e", b)].wait()
        part = jnp.dot(ms[...].astype(BF16), ev[b], preferred_element_type=F32)
        for j in range(n_dp):
            psend[b, j] = part[j * PAD : j * PAD + rows].astype(BF16)
        if b < blocks - 1:
            shared = []
            for k in range(1, n_tp):
                copy = remote(psend.at[b], precv.at[b, k - 1], peer(tp_to(k), dp))
                copy.start()
                shared.append(copy)
            for copy in shared:
                copy.wait_recv()
            outgoing += shared
            for j in range(n_dp):
                at = j * PAD
                total = part[at : at + rows]
                for k in range(1, n_tp):
                    total = total + precv[b, k - 1, j].astype(F32)
                xs[at : at + rows, :] = (x_now[at : at + rows] + total).astype(BF16).astype(F32)
        else:
            pown[:, 0:feats] = part
            shared = []
            for k in range(1, n_tp):
                copy = remote(
                    psend.at[b, pl.ds(tp_to(k) * per_tp, per_tp)],
                    precv.at[b, k - 1, pl.ds(0, per_tp)],
                    peer(tp_to(k), dp),
                )
                copy.start()
                shared.append(copy)
            for copy in shared:
                copy.wait_recv()
            outgoing += shared
            pieces = []
            for g in range(per_tp):
                at = pl.multiple_of((tp * per_tp + g) * PAD, PAD)
                total = pown[pl.ds(at, PAD), 0:feats][0:rows]
                for k in range(1, n_tp):
                    total = total + precv[b, k - 1, g].astype(F32)
                pieces.append(sequence_major(xs[pl.ds(at, PAD), :][0:rows] + total))
            out_ref[...] = jnp.concatenate(pieces, axis=0).astype(BF16)

    for copy in outgoing:
        copy.wait_send()


def store_kernel(out_vmem, state_vmem, out_hbm, state_hbm, sem):
    copies = [
        pltpu.make_async_copy(state_vmem, state_hbm, sem.at[0]),
        pltpu.make_async_copy(out_vmem, out_hbm, sem.at[1]),
    ]
    for copy in copies:
        copy.start()
    for copy in copies:
        copy.wait()


def solution(mesh):
    n_tp, n_dp = mesh.shape["tp"], mesh.shape["dp"]

    def shards(
        hidden,
        live,
        gain,
        w0,
        w1,
        w2,
        w3,
        w4,
        w5,
        ceiling,
        rescale,
        exit_w,
        memories,
        fade,
    ):
        blocks, feats, chans = w0.shape
        seqs, heads, size = memories.shape[1], memories.shape[2], memories.shape[3]
        rows = fade.shape[1]
        nz = n_dp // 2
        width = 3 * chans + EXTRA
        copies = (n_tp - 1) * (1 + blocks) + blocks * (3 + 2 * (n_dp - 1))
        outputs = 4 * blocks * seqs * heads * size * (-(-size // LANES) * LANES)
        outputs += 4 * hidden.shape[0] * hidden.shape[1]
        vmem = pl.BlockSpec(memory_space=pltpu.VMEM)
        smem = pl.BlockSpec(memory_space=pltpu.SMEM)
        hbm = pl.BlockSpec(memory_space=pl.ANY)
        placed = pl.pallas_call(
            functools.partial(kernel, n_tp, n_dp),
            out_shape=(
                pltpu.VMEM(hidden.shape, hidden.dtype),
                pltpu.VMEM(memories.shape, memories.dtype),
            ),
            in_specs=[hbm, smem] + [hbm] * 12,
            out_specs=(vmem, vmem),
            scratch_shapes=[
                pltpu.VMEM((blocks, 6, feats, chans), BF16),
                pltpu.VMEM((blocks, chans, feats), BF16),
                pltpu.VMEM((blocks, seqs, heads, size, size), F32),
                pltpu.VMEM((n_tp,) + hidden.shape, BF16),
                pltpu.VMEM((n_dp * PAD, feats), F32),
                pltpu.VMEM((n_dp * PAD, chans), F32),
                pltpu.VMEM((n_dp * PAD, 3 * chans), F32),
                pltpu.VMEM((blocks, n_dp, rows, width), BF16),
                pltpu.VMEM((blocks, n_dp, rows, width), BF16),
                pltpu.VMEM((blocks, n_dp, rows, width), BF16),
                pltpu.VMEM((blocks, nz, 2, rows, width), BF16),
                pltpu.VMEM((PAD, 6 * chans), F32),
                pltpu.VMEM((blocks, n_dp, rows, chans), BF16),
                pltpu.VMEM((blocks, n_dp, rows, feats), BF16),
                pltpu.VMEM((blocks, n_tp - 1, n_dp, rows, feats), BF16),
                pltpu.VMEM(gain.shape, BF16),
                pltpu.VMEM(ceiling.shape, F32),
                pltpu.VMEM(rescale.shape, F32),
                pltpu.VMEM((rows, blocks, fade.shape[2]), F32),
                pltpu.VMEM((seqs, heads * size, size), BF16),
                pltpu.VMEM((seqs, heads * size, size), BF16),
                pltpu.SemaphoreType.DMA((blocks * 8 + 5,)),
                pltpu.SemaphoreType.DMA((blocks,)),
                pltpu.SemaphoreType.DMA((copies,)),
                pltpu.SemaphoreType.DMA((copies,)),
            ],
            compiler_params=pltpu.CompilerParams(
                collective_id=0, has_side_effects=True, vmem_limit_bytes=VMEM_BYTES - outputs
            ),
        )(hidden, live, gain, w0, w1, w2, w3, w4, w5, ceiling, rescale, exit_w, memories, fade.transpose(1, 0, 2))
        return pl.pallas_call(
            store_kernel,
            out_shape=(
                jax.ShapeDtypeStruct(hidden.shape, hidden.dtype),
                jax.ShapeDtypeStruct(memories.shape, memories.dtype),
            ),
            in_specs=[vmem, vmem],
            out_specs=(hbm, hbm),
            scratch_shapes=[pltpu.SemaphoreType.DMA((2,))],
            compiler_params=pltpu.CompilerParams(vmem_limit_bytes=1048576),
        )(*placed)

    in_specs = (
        P("tp", "dp"),
        P("dp"),
        P(None, "dp"),
        P(None, "dp", "tp"),
        P(None, "dp", "tp"),
        P(None, "dp", "tp"),
        P(None, "dp", "tp"),
        P(None, "dp", "tp"),
        P(None, "dp", "tp"),
        P(None, "tp"),
        P(None, "tp"),
        P(None, "tp", "dp"),
        P(None, "dp", "tp", None, None),
        P(None, "dp", "tp"),
    )
    out_specs = (P("tp", "dp"), P(None, "dp", "tp", None, None))
    return jax.shard_map(shards, mesh=mesh, in_specs=in_specs, out_specs=out_specs, check_vma=False)
```

```python
import functools

import jax
import jax.numpy as jnp
from jax import lax
from jax.experimental import pallas as pl
from jax.experimental.pallas import tpu as pltpu
from jax.sharding import PartitionSpec as P

NORM_EPS = 1e-06
KEY_EPS = 1e-06
GROUP_EPS = 0.00064
PAD = 8
LANES = 128
WIDEST = 256
VMEM_BYTES = 67043328
F32 = jnp.float32
BF16 = jnp.bfloat16


def packing(tiles, rows, extra):
    spare = PAD - rows
    kept = next(k for k in range(1, tiles + 2) if k * spare >= max(tiles - k, 0) * rows + extra)
    kept = max(kept, 1)
    stream = [(u, r) for u in range(kept, tiles) for r in range(rows)]
    stream += [(None, r) for r in range(extra)]
    return kept, [stream[t * spare : (t + 1) * spare] for t in range(kept)]


def runs(slots):
    found = []
    for at, (u, r) in enumerate(slots):
        if found and found[-1][0] == u and found[-1][2] == r:
            found[-1][2] = r + 1
        else:
            found.append([u, r, r + 1, at])
    return found


def pack(tiles, rows, extra):
    kept, slots = packing(len(tiles), rows, len(extra))
    packed = []
    for t in range(kept):
        parts = [tiles[t][0:rows] if t < len(tiles) else jnp.zeros((rows, LANES), F32)]
        for u, first, last, at in runs(slots[t]):
            parts += extra[first:last] if u is None else [tiles[u][first:last]]
        missing = PAD - rows - len(slots[t])
        if missing:
            parts.append(jnp.zeros((missing, LANES), F32))
        packed.append(jnp.concatenate(parts, axis=0))
    return jnp.concatenate(packed, axis=1)


def unpack(packed, tiles, rows, extra):
    kept, slots = packing(tiles, rows, extra)
    cut = [packed[:, t * LANES : (t + 1) * LANES] for t in range(kept)]
    moved, found = {}, []
    for t in range(kept):
        for u, first, last, at in runs(slots[t]):
            piece = cut[t][rows + at : rows + at + last - first]
            if u is None:
                found += [piece[i : i + 1] for i in range(last - first)]
            else:
                moved.setdefault(u, []).append(piece)
    for u in range(kept, tiles):
        parts = moved[u] + [jnp.zeros((PAD - rows, LANES), F32)]
        cut.append(jnp.concatenate(parts, axis=0))
    return jnp.concatenate(cut[:tiles], axis=1), found


def pieces_of(groups):
    pieces = []
    for g in range(groups):
        pieces += [(g, True, (0,)), (g, False, (1, 2))] if g == 0 else [
            (g, False, (0, 1)),
            (g, False, (2,)),
        ]
    return pieces


def piece_shape(piece, per_proj):
    g, whole, kinds = piece
    return len(kinds) * per_proj * (2 if whole else 1), 2 if whole else 0


def kernel(
    n_tp,
    n_dp,
    x_hbm,
    live_ref,
    gain_hbm,
    w0,
    w1,
    w2,
    w3,
    w4,
    w5,
    ceiling_hbm,
    rescale_hbm,
    exit_hbm,
    memory_hbm,
    fade_hbm,
    out_ref,
    state_ref,
    wv,
    ev,
    mem,
    gx,
    xs,
    pown,
    dsend,
    drecv,
    mbuf,
    psend,
    precv,
    gain_ref,
    ceiling_ref,
    rescale_ref,
    fade_ref,
    s_cat,
    load_sem,
    send_sem,
    recv_sem,
    *piece_refs,
):
    blocks = wv.shape[0]
    feats = x_hbm.shape[1]
    seqs, heads, size = mem.shape[1], mem.shape[2], mem.shape[3]
    rows = fade_hbm.shape[0]
    steps = rows // seqs
    groups, wide = mbuf.shape[1], mbuf.shape[4]
    together = heads // groups
    nz = n_dp // 2
    per_tp = n_dp // n_tp
    per_proj = wide // LANES
    pieces = pieces_of(groups)
    zsend, zrecv = piece_refs[0::2], piece_refs[1::2]
    feat_tiles = feats // LANES

    tp = lax.axis_index("tp")
    dp = lax.axis_index("dp")
    z = dp // 2
    core = dp % 2
    other = 1 - core

    def peer(tp_at, dp_at):
        return {"tp": tp_at, "dp": dp_at}

    def tp_to(m):
        at, bit = tp * 0, 1
        while bit < n_tp:
            mine = (tp // bit) % 2
            at = at + bit * ((1 - mine) if m & bit else mine)
            bit *= 2
        return at

    def dp_to(dz, flip):
        return lax.rem(z + dz, nz) * 2 + (other if flip else core)

    tp_offsets = sorted(range(1, n_tp), key=lambda m: -bin(m).count("1"))
    dp_offsets = [(dz, f) for dz in range(nz) for f in range(2) if (dz, f) != (0, 0)]
    far_first = sorted(dp_offsets, key=lambda o: -min(o[0], nz - o[0]))

    def slot_major(values):
        return jnp.concatenate(
            [
                values[s * steps + t : s * steps + t + 1]
                for t in range(steps)
                for s in range(seqs)
            ],
            axis=0,
        )

    def sequence_major(values):
        return jnp.concatenate(
            [
                values[t * seqs + s : t * seqs + s + 1]
                for s in range(seqs)
                for t in range(steps)
            ],
            axis=0,
        )

    counter = [0]

    def remote(src, dst, to, lands=None):
        at = counter[0]
        counter[0] += 1

        def copy(dst_ref):
            return pltpu.make_async_remote_copy(
                src_ref=src,
                dst_ref=dst_ref,
                send_sem=send_sem.at[at],
                recv_sem=recv_sem.at[at],
                device_id=to,
                device_id_type=pl.DeviceIdType.MESH,
            )

        sent = copy(dst)
        sent.start()
        outgoing.append(sent)
        return sent if lands is None else copy(lands)

    outgoing = []
    weights = (w1, w0, w2, w3, w4, w5)
    loads = {}

    def load(name, src, dst):
        copy = pltpu.make_async_copy(src, dst, load_sem.at[len(loads)])
        copy.start()
        loads[name] = copy

    load("x", x_hbm, gx.at[tp])
    load("gain", gain_hbm, gain_ref)
    load("ceiling", ceiling_hbm, ceiling_ref)
    load("rescale", rescale_hbm, rescale_ref)
    load("fade", fade_hbm, fade_ref)
    for b in range(blocks):
        for p in range(6):
            load(("w", b, p), weights[p].at[b], wv.at[b, p])
        load(("m", b), memory_hbm.at[b], mem.at[b])
        load(("e", b), exit_hbm.at[b], ev.at[b])

    barrier = pltpu.get_barrier_semaphore()
    for m in tp_offsets:
        pl.semaphore_signal(
            barrier, inc=1, device_id=peer(tp_to(m), dp), device_id_type=pl.DeviceIdType.MESH
        )
    for dz, f in far_first:
        pl.semaphore_signal(
            barrier, inc=1, device_id=peer(tp, dp_to(dz, f)), device_id_type=pl.DeviceIdType.MESH
        )
    xs[...] = jnp.zeros_like(xs)
    loads["x"].wait()
    pl.semaphore_wait(barrier, n_tp - 1 + len(dp_offsets))

    first = []
    for m in tp_offsets:
        first.append(remote(gx.at[tp], gx.at[tp], peer(tp_to(m), dp), gx.at[tp_to(m)]))

    row_at = lax.broadcasted_iota(jnp.int32, (PAD, 1), 0)
    live_col = jnp.zeros((PAD, 1), F32)
    for s in range(seqs):
        for t in range(steps):
            live_col = jnp.where(
                row_at == t * seqs + s, jnp.where(live_ref[s] > t, 1.0, 0.0), live_col
            )
    live3 = [
        live_col[t * seqs : (t + 1) * seqs].reshape(1, seqs, 1) for t in range(steps)
    ]
    on_row = lax.broadcasted_iota(jnp.int32, (n_dp * PAD, LANES), 1) == (
        lax.broadcasted_iota(jnp.int32, (n_dp * PAD, LANES), 0) % PAD
    )
    kinds = 2 * steps * seqs
    deep = -(-kinds // 16) * 16
    kind_at = lax.broadcasted_iota(jnp.int32, (together * deep, 1), 0) % deep % seqs
    slot_at = lax.broadcasted_iota(jnp.int32, (3 * deep, 1), 0) % deep % seqs
    filler = [jnp.zeros((together, deep - kinds, size), F32)] * (deep > kinds)

    def split_states(b):
        loads[("m", b)].wait()
        for s in range(seqs):
            state = mem[b, s].reshape(heads * size, size)
            high = state.astype(BF16)
            low = (state - high.astype(F32)).astype(BF16)
            s_cat[b, s, :, 0:size] = high
            s_cat[b, s, :, size : 2 * size] = high
            s_cat[b, s, :, 2 * size : 3 * size] = low

    for name in ("gain", "ceiling", "rescale", "fade"):
        loads[name].wait()
    split_states(0)
    for p in range(6):
        loads[("w", 0, p)].wait()
    for copy in first:
        copy.wait_recv()
    for i in range(n_tp):
        whole = gx[i].astype(F32)
        for g in range(per_tp):
            xs[(i * per_tp + g) * PAD : (i * per_tp + g) * PAD + rows, :] = slot_major(
                whole[g * rows : (g + 1) * rows]
            )

    for b in range(blocks):
        x_now = xs[...]
        gained = (x_now * gain_ref[b : b + 1, :].astype(F32)).astype(BF16)

        def project(slots, g):
            return jnp.concatenate(
                [
                    jnp.dot(
                        gained,
                        wv[b, p, :, g * wide : (g + 1) * wide],
                        preferred_element_type=F32,
                    )
                    for p in slots
                ],
                axis=1,
            )

        scattered = {}

        def scatter(i, values):
            tiles, extra = piece_shape(pieces[i], per_proj)
            for j in range(n_dp):
                block = values[j * PAD : (j + 1) * PAD]
                cut = [block[:, t * LANES : (t + 1) * LANES] for t in range(tiles)]
                noted = [lined_high[j : j + 1], lined_low[j : j + 1]] if extra else []
                zsend[i][b, j] = pack(cut, rows, noted).astype(BF16)
            ways = []
            for dz, f in far_first:
                to = dp_to(dz, f)
                ways.append(
                    remote(
                        zsend[i].at[b, to],
                        zrecv[i].at[b, dz, core],
                        peer(tp, to),
                        zrecv[i].at[b, dz, other if f else core],
                    )
                )
            scattered[i] = ways

        halves = [
            sorted(k for g_at, whole, kinds in pieces if g_at == g and not whole for k in kinds)
            for g in range(groups)
        ]
        pairs, own = [], []

        def give(g):
            width = len(halves[g]) * wide
            dsend[b, g, :, 0:width] = project([3 * other + k for k in halves[g]], g).astype(BF16)
            pairs.append(
                remote(
                    dsend.at[b, g, :, pl.ds(0, width)],
                    drecv.at[b, g, :, pl.ds(0, width)],
                    peer(tp, dp_to(0, 1)),
                )
            )

        give(0)
        squares = jnp.sum(x_now * x_now, axis=1, keepdims=True)
        lined = jnp.where(on_row, squares, 0.0).reshape(n_dp, PAD, LANES)
        lined = jnp.sum(lined, axis=1)
        lined_high = lined.astype(BF16).astype(F32)
        lined_low = lined - lined_high
        for i, (g, whole, kinds) in enumerate(pieces):
            if whole:
                scatter(i, project([3 * h + k for h in range(2) for k in kinds], g))
        for g in range(1, groups):
            give(g)
        for g in range(groups):
            own.append(project([3 * core + k for k in halves[g]], g))
        for g in range(groups):
            pairs[g].wait_recv()
            both = own[g] + drecv[b, g, :, 0 : len(halves[g]) * wide].astype(F32)
            for i, (g_at, whole, kinds) in enumerate(pieces):
                if g_at == g and not whole:
                    at = halves[g].index(kinds[0]) * wide
                    scatter(i, both[:, at : at + len(kinds) * wide])
        for i in range(len(pieces)):
            zrecv[i][b, 0, core] = zsend[i][b, dp]
        if b > 0:
            split_states(b)
        fade_b = slot_major(fade_ref[:, b, :])
        fade_b = jnp.concatenate([fade_b, jnp.zeros((PAD - rows, heads), F32)], axis=0)
        row_scale = None

        gathered, later = [], []
        for g in range(groups):
            values = {}

            def arrive(slot):
                nonlocal row_scale
                i = next(
                    i
                    for i, (g_at, whole, kinds) in enumerate(pieces)
                    if g_at == g and slot % 3 in kinds
                )
                whole, kinds = pieces[i][1:]
                tiles, extra = piece_shape(pieces[i], per_proj)
                for way in reversed(scattered[i]):
                    way.wait_recv()
                sums = []
                for h in range(2):
                    total = zrecv[i][b, 0, h].astype(F32)
                    for dz in range(1, nz):
                        total = total + zrecv[i][b, dz, h].astype(F32)
                    sums.append(total)
                named = [[3 * h + k for k in kinds] for h in range(2)]
                if whole:
                    sums, named = [sums[0] + sums[1]], [named[0] + named[1]]
                for total, names in zip(sums, named):
                    total, noted = unpack(total, tiles, rows, extra)
                    if noted:
                        line = sum(noted[1:], noted[0])
                        total_squares = jnp.sum(
                            jnp.where(on_row[0:PAD], line, 0.0), axis=1, keepdims=True
                        )
                        row_scale = lax.rsqrt(total_squares / (feats * n_dp) + NORM_EPS)
                    for n, name in enumerate(names):
                        values[name] = total[:, n * wide : (n + 1) * wide] * row_scale

            def flat(slot):
                if slot not in values:
                    arrive(slot)
                return values[slot]

            def by_head(slot):
                rows_now = flat(slot)
                return jnp.stack(
                    [rows_now[:, h * size : (h + 1) * size] for h in range(together)]
                )

            def slots(values):
                return [values[:, t * seqs : (t + 1) * seqs, :] for t in range(steps)]

            key3, fade3 = by_head(0), by_head(3)
            ceiling = ceiling_ref[b : b + 1, g * wide : (g + 1) * wide]
            decay3 = jnp.stack(
                [
                    jnp.exp(
                        fade_b[:, g * together + h : g * together + h + 1]
                        - ceiling[:, h * size : (h + 1) * size] * jax.nn.sigmoid(fade3[h])
                    )
                    for h in range(together)
                ]
            )
            unit3 = key3 * lax.rsqrt(jnp.sum(key3 * key3, axis=2, keepdims=True) + KEY_EPS)
            key, decay, unit = slots(key3), slots(decay3), slots(unit3)
            read = slots(by_head(1))

            wanted = []
            before = None
            for t in range(steps):
                wanted.append(unit[t] if before is None else before * unit[t])
                before = decay[t] if before is None else before * decay[t]
                wanted.append(before * read[t])
            wanted = jnp.concatenate(wanted + filler, axis=1).reshape(together * deep, size)
            wanted_high = wanted.astype(BF16).astype(F32)
            lhs = jnp.concatenate(
                [wanted_high, wanted - wanted_high, wanted_high], axis=1
            ).astype(BF16)
            found = None
            for s in range(seqs):
                product = lax.dot_general(
                    lhs,
                    s_cat[b, s, g * wide : (g + 1) * wide, :],
                    (((1,), (1,)), ((), ())),
                    preferred_element_type=F32,
                )
                found = product if found is None else jnp.where(kind_at == s, product, found)
            found3 = jnp.stack(
                [
                    found[h * deep : (h + 1) * deep, h * size : (h + 1) * size]
                    for h in range(together)
                ]
            )
            pull = slots(unit3 * jax.nn.sigmoid(by_head(4)))
            value = slots(by_head(2))
            base = [found3[:, i * seqs : (i + 1) * seqs, :] for i in range(2 * steps)]

            def dot3(a, c):
                return jnp.sum(a * c, axis=2, keepdims=True)

            taken = []

            def state_times(count, start, vector):
                total = start
                for i in range(count - 1, -1, -1):
                    total = (
                        total - dot3(pull[i], vector) * taken[i] + dot3(key[i], vector) * value[i]
                    )
                    if i:
                        vector = decay[i] * vector
                return total

            readouts = []
            for t in range(steps):
                taken.append(state_times(t, base[2 * t], unit[t]))
                readouts.append(state_times(t + 1, base[2 * t + 1], read[t]))
            readout = jnp.concatenate(readouts, axis=1)
            centered = readout - jnp.mean(readout, axis=2, keepdims=True)
            normed = centered * lax.rsqrt(
                jnp.mean(centered * centered, axis=2, keepdims=True) + GROUP_EPS
            )
            normed_rows = jnp.concatenate([normed[h] for h in range(together)], axis=1)
            gate = jax.nn.sigmoid(flat(5)[0:rows])
            rescale = rescale_ref[b : b + 1, g * wide : (g + 1) * wide]
            mixed = normed_rows * rescale * gate * live_col[0:rows]
            mixed = jnp.concatenate([mixed, jnp.zeros((PAD - rows, wide), F32)], axis=0)
            mbuf[b, g, dp] = mixed.astype(BF16)
            ways = []
            for dz, f in far_first:
                to = dp_to(dz, f)
                ways.append(
                    remote(mbuf.at[b, g, dp], mbuf.at[b, g, dp], peer(tp, to), mbuf.at[b, g, to])
                )
            gathered.append(ways)
            later.append((taken, value, pull, key, decay))

        for g in range(groups):
            taken, value, pull, key, decay = later[g]
            left, right = [], []
            after = None
            for t in range(steps - 1, -1, -1):
                left += [-taken[t] * live3[t], value[t] * live3[t]]
                right += [pull[t] if after is None else pull[t] * after]
                right += [key[t] if after is None else key[t] * after]
                kept = jnp.where(live3[t] > 0.0, decay[t], 1.0)
                after = kept if after is None else after * kept
            left = jnp.concatenate(left + filler, axis=1)
            right = jnp.concatenate(right + filler, axis=1)
            left_high = left.astype(BF16).astype(F32)
            right_high = right.astype(BF16).astype(F32)
            left = jnp.concatenate([left_high, left - left_high, left_high], axis=1).astype(BF16)
            right = jnp.concatenate([right_high, right_high, right - right_high], axis=1)
            for s in range(seqs):
                for h in range(together):
                    at = g * together + h
                    mine = jnp.where(slot_at == s, right[h], 0.0).astype(BF16)
                    state_ref[b, s, at] = mem[b, s, at] * after[h, s : s + 1, :] + lax.dot_general(
                        left[h], mine, (((0,), (0,)), ((), ())), preferred_element_type=F32
                    )

        loads[("e", b)].wait()
        if b < blocks - 1:
            for p in range(6):
                loads[("w", b + 1, p)].wait()
        part = None
        for g in range(groups):
            for way in reversed(gathered[g]):
                way.wait_recv()
            lhs = mbuf[b, g].astype(F32).reshape(n_dp * PAD, wide).astype(BF16)
            product = jnp.dot(
                lhs, ev[b, g * wide : (g + 1) * wide, :], preferred_element_type=F32
            )
            part = product if part is None else part + product
        for j in range(n_dp):
            block = part[j * PAD : (j + 1) * PAD]
            tiles = [block[:, t * LANES : (t + 1) * LANES] for t in range(feat_tiles)]
            psend[b, j] = pack(tiles, rows, []).astype(BF16)
        shared = []
        if b < blocks - 1:
            for i, m in enumerate(tp_offsets):
                shared.append(remote(psend.at[b], precv.at[b, i], peer(tp_to(m), dp)))
            for copy in shared:
                copy.wait_recv()
            for j in range(n_dp):
                at = j * PAD
                total = precv[b, 0, j].astype(F32)
                for i in range(1, n_tp - 1):
                    total = total + precv[b, i, j].astype(F32)
                total, extra = unpack(total, feat_tiles, rows, 0)
                total = total + part[at : at + PAD]
                xs[at : at + PAD, :] = (x_now[at : at + PAD] + total).astype(BF16).astype(F32)
        else:
            pown[...] = x_now + part
            for i, m in enumerate(tp_offsets):
                to = tp_to(m)
                shared.append(
                    remote(
                        psend.at[b, pl.ds(to * per_tp, per_tp)],
                        precv.at[b, i, pl.ds(0, per_tp)],
                        peer(to, dp),
                    )
                )
            for copy in shared:
                copy.wait_recv()
            pieces = []
            for g in range(per_tp):
                at = pl.multiple_of((tp * per_tp + g) * PAD, PAD)
                total = precv[b, 0, g].astype(F32)
                for i in range(1, n_tp - 1):
                    total = total + precv[b, i, g].astype(F32)
                total, extra = unpack(total, feat_tiles, rows, 0)
                pieces.append(sequence_major((pown[pl.ds(at, PAD), :] + total)[0:rows]))
            out_ref[...] = jnp.concatenate(pieces, axis=0).astype(BF16)

    for copy in outgoing:
        copy.wait_send()


def store_kernel(out_vmem, state_vmem, out_hbm, state_hbm, sem):
    copies = [
        pltpu.make_async_copy(state_vmem, state_hbm, sem.at[0]),
        pltpu.make_async_copy(out_vmem, out_hbm, sem.at[1]),
    ]
    for copy in copies:
        copy.start()
    for copy in copies:
        copy.wait()


def solution(mesh):
    n_tp, n_dp = mesh.shape["tp"], mesh.shape["dp"]

    def shards(
        hidden,
        live,
        gain,
        w0,
        w1,
        w2,
        w3,
        w4,
        w5,
        ceiling,
        rescale,
        exit_w,
        memories,
        fade,
    ):
        blocks, feats, chans = w0.shape
        seqs, heads, size = memories.shape[1], memories.shape[2], memories.shape[3]
        rows = fade.shape[1]
        nz = n_dp // 2
        together = max(d for d in range(1, heads + 1) if heads % d == 0 and d * size <= WIDEST)
        groups, wide = heads // together, together * size
        pieces = pieces_of(groups)
        shapes = [piece_shape(piece, wide // LANES) for piece in pieces]
        packed = [LANES * packing(tiles, rows, extra)[0] for tiles, extra in shapes]
        sent = LANES * packing(feats // LANES, rows, 0)[0]
        copies = (n_tp - 1) * (1 + blocks) + blocks * groups
        copies += blocks * (groups + len(pieces)) * (n_dp - 1)
        outputs = 4 * blocks * seqs * heads * size * (-(-size // LANES) * LANES)
        outputs += 4 * hidden.shape[0] * hidden.shape[1]
        vmem = pl.BlockSpec(memory_space=pltpu.VMEM)
        smem = pl.BlockSpec(memory_space=pltpu.SMEM)
        hbm = pl.BlockSpec(memory_space=pl.ANY)
        placed = pl.pallas_call(
            functools.partial(kernel, n_tp, n_dp),
            out_shape=(
                pltpu.VMEM(hidden.shape, hidden.dtype),
                pltpu.VMEM(memories.shape, memories.dtype),
            ),
            in_specs=[hbm, smem] + [hbm] * 12,
            out_specs=(vmem, vmem),
            scratch_shapes=[
                pltpu.VMEM((blocks, 6, feats, chans), BF16),
                pltpu.VMEM((blocks, chans, feats), BF16),
                pltpu.VMEM((blocks, seqs, heads, size, size), F32),
                pltpu.VMEM((n_tp,) + hidden.shape, BF16),
                pltpu.VMEM((n_dp * PAD, feats), F32),
                pltpu.VMEM((n_dp * PAD, feats), F32),
                pltpu.VMEM((blocks, groups, n_dp * PAD, 3 * wide), BF16),
                pltpu.VMEM((blocks, groups, n_dp * PAD, 3 * wide), BF16),
                pltpu.VMEM((blocks, groups, n_dp, PAD, wide), BF16),
                pltpu.VMEM((blocks, n_dp, PAD, sent), BF16),
                pltpu.VMEM((blocks, n_tp - 1, n_dp, PAD, sent), BF16),
                pltpu.VMEM(gain.shape, BF16),
                pltpu.VMEM(ceiling.shape, F32),
                pltpu.VMEM(rescale.shape, F32),
                pltpu.VMEM((rows, blocks, fade.shape[2]), F32),
                pltpu.VMEM((blocks, seqs, heads * size, 3 * size), BF16),
                pltpu.SemaphoreType.DMA((blocks * 8 + 5,)),
                pltpu.SemaphoreType.DMA((copies,)),
                pltpu.SemaphoreType.DMA((copies,)),
            ]
            + [
                pltpu.VMEM((blocks,) + shape + (PAD, width), BF16)
                for width in packed
                for shape in ((n_dp,), (nz, 2))
            ],
            compiler_params=pltpu.CompilerParams(
                collective_id=0, has_side_effects=True, vmem_limit_bytes=VMEM_BYTES - outputs
            ),
        )(hidden, live, gain, w0, w1, w2, w3, w4, w5, ceiling, rescale, exit_w, memories, fade.transpose(1, 0, 2))
        return pl.pallas_call(
            store_kernel,
            out_shape=(
                jax.ShapeDtypeStruct(hidden.shape, hidden.dtype),
                jax.ShapeDtypeStruct(memories.shape, memories.dtype),
            ),
            in_specs=[vmem, vmem],
            out_specs=(hbm, hbm),
            scratch_shapes=[pltpu.SemaphoreType.DMA((2,))],
            compiler_params=pltpu.CompilerParams(vmem_limit_bytes=1048576),
        )(*placed)

    in_specs = (
        P("tp", "dp"),
        P("dp"),
        P(None, "dp"),
        P(None, "dp", "tp"),
        P(None, "dp", "tp"),
        P(None, "dp", "tp"),
        P(None, "dp", "tp"),
        P(None, "dp", "tp"),
        P(None, "dp", "tp"),
        P(None, "tp"),
        P(None, "tp"),
        P(None, "tp", "dp"),
        P(None, "dp", "tp", None, None),
        P(None, "dp", "tp"),
    )
    out_specs = (P("tp", "dp"), P(None, "dp", "tp", None, None))
    return jax.shard_map(shards, mesh=mesh, in_specs=in_specs, out_specs=out_specs, check_vma=False)
```

```python
import functools

import jax
import jax.numpy as jnp
from jax import lax
from jax.experimental import pallas as pl
from jax.experimental.pallas import tpu as pltpu
from jax.sharding import PartitionSpec as P

NORM_EPS = 1e-06
KEY_EPS = 1e-06
GROUP_EPS = 0.00064
PAD = 8
LANES = 128
WIDEST = 256
VMEM_BYTES = 67043328
F32 = jnp.float32
BF16 = jnp.bfloat16


def packing(tiles, rows, extra):
    spare = PAD - rows
    kept = next(k for k in range(1, tiles + 2) if k * spare >= max(tiles - k, 0) * rows + extra)
    kept = max(kept, 1)
    stream = [(u, r) for u in range(kept, tiles) for r in range(rows)]
    stream += [(None, r) for r in range(extra)]
    return kept, [stream[t * spare : (t + 1) * spare] for t in range(kept)]


def runs(slots):
    found = []
    for at, (u, r) in enumerate(slots):
        if found and found[-1][0] == u and found[-1][2] == r:
            found[-1][2] = r + 1
        else:
            found.append([u, r, r + 1, at])
    return found


def pack(tiles, rows, extra):
    kept, slots = packing(len(tiles), rows, len(extra))
    packed = []
    for t in range(kept):
        parts = [tiles[t][0:rows] if t < len(tiles) else jnp.zeros((rows, LANES), F32)]
        for u, first, last, at in runs(slots[t]):
            parts += extra[first:last] if u is None else [tiles[u][first:last]]
        missing = PAD - rows - len(slots[t])
        if missing:
            parts.append(jnp.zeros((missing, LANES), F32))
        packed.append(jnp.concatenate(parts, axis=0))
    return jnp.concatenate(packed, axis=1)


def unpack(packed, tiles, rows, extra):
    kept, slots = packing(tiles, rows, extra)
    cut = [packed[:, t * LANES : (t + 1) * LANES] for t in range(kept)]
    moved, found = {}, []
    for t in range(kept):
        for u, first, last, at in runs(slots[t]):
            piece = cut[t][rows + at : rows + at + last - first]
            if u is None:
                found += [piece[i : i + 1] for i in range(last - first)]
            else:
                moved.setdefault(u, []).append(piece)
    for u in range(kept, tiles):
        parts = moved[u] + [jnp.zeros((PAD - rows, LANES), F32)]
        cut.append(jnp.concatenate(parts, axis=0))
    return jnp.concatenate(cut[:tiles], axis=1), found


def pieces_of(groups):
    pieces = []
    for g in range(groups):
        pieces += [(g, True, (0,)), (g, False, (1, 2))] if g == 0 else [
            (g, False, (0, 1)),
            (g, False, (2,)),
        ]
    return pieces


def piece_shape(piece, per_proj):
    g, whole, kinds = piece
    return len(kinds) * per_proj * (2 if whole else 1)


def kernel(
    n_tp,
    n_dp,
    x_hbm,
    live_ref,
    gain_hbm,
    w0,
    w1,
    w2,
    w3,
    w4,
    w5,
    ceiling_hbm,
    rescale_hbm,
    exit_hbm,
    memory_hbm,
    fade_hbm,
    out_ref,
    state_ref,
    wv,
    ev,
    mem,
    gx,
    xs,
    pown,
    dsend,
    drecv,
    mbuf,
    psend,
    precv,
    qsend,
    qrecv,
    gain_ref,
    ceiling_ref,
    rescale_ref,
    fade_ref,
    s_cat,
    load_sem,
    send_sem,
    recv_sem,
    *piece_refs,
):
    blocks = wv.shape[0]
    feats = x_hbm.shape[1]
    seqs, heads, size = mem.shape[1], mem.shape[2], mem.shape[3]
    rows = fade_hbm.shape[0]
    steps = rows // seqs
    groups, wide = mbuf.shape[1], mbuf.shape[4]
    together = heads // groups
    nz = n_dp // 2
    per_tp = n_dp // n_tp
    per_proj = wide // LANES
    pieces = pieces_of(groups)
    zsend, zrecv = piece_refs[0::2], piece_refs[1::2]
    cuts, dests = psend.shape[1], n_dp // psend.shape[2]
    cut_feats = feats // cuts
    cut_tiles = cut_feats // LANES

    tp = lax.axis_index("tp")
    dp = lax.axis_index("dp")
    z = dp // 2
    core = dp % 2
    other = 1 - core

    def peer(tp_at, dp_at):
        return {"tp": tp_at, "dp": dp_at}

    def tp_to(m):
        at, bit = tp * 0, 1
        while bit < n_tp:
            mine = (tp // bit) % 2
            at = at + bit * ((1 - mine) if m & bit else mine)
            bit *= 2
        return at

    sibling = z * 2 + other
    far = [sorted(range(nz), key=lambda at: -abs(at - i)) for i in range(nz)]
    far_z = [sum(jnp.where(z == i, far[i][k], 0) for i in range(nz)) for k in range(nz - 1)]
    dp_others = [at * 2 + c for at in far_z for c in (core, other)] + [sibling]

    tp_offsets = sorted(range(1, n_tp), key=lambda m: -bin(m).count("1"))

    def slot_major(values):
        return jnp.concatenate(
            [
                values[s * steps + t : s * steps + t + 1]
                for t in range(steps)
                for s in range(seqs)
            ],
            axis=0,
        )

    def sequence_major(values):
        return jnp.concatenate(
            [
                values[t * seqs + s : t * seqs + s + 1]
                for s in range(seqs)
                for t in range(steps)
            ],
            axis=0,
        )

    counter = [0]

    def remote(src, dst, to, lands=None):
        at = counter[0]
        counter[0] += 1

        def copy(dst_ref):
            return pltpu.make_async_remote_copy(
                src_ref=src,
                dst_ref=dst_ref,
                send_sem=send_sem.at[at],
                recv_sem=recv_sem.at[at],
                device_id=to,
                device_id_type=pl.DeviceIdType.MESH,
            )

        sent = copy(dst)
        sent.start()
        outgoing.append(sent)
        return sent if lands is None else copy(lands)

    def spread(src_for, dst_of):
        at = counter[0]
        counter[0] += n_dp

        def copy(k, to, dst_ref, source):
            return pltpu.make_async_remote_copy(
                src_ref=src_for(to),
                dst_ref=dst_ref,
                send_sem=send_sem.at[at + k],
                recv_sem=recv_sem.at[at + source],
                device_id=peer(tp, to),
                device_id_type=pl.DeviceIdType.MESH,
            )

        for k, to in enumerate(dp_others):
            sent = copy(k, to, dst_of(dp), dp)
            sent.start()
            outgoing.append(sent)
        return [copy(k, to, dst_of(to), to) for k, to in enumerate(dp_others)]

    outgoing = []

    def flush(count):
        for copy in outgoing[:count]:
            copy.wait_send()
        del outgoing[:count]

    weights = (w1, w0, w2, w3, w4, w5)
    loads = {}

    def load(name, src, dst):
        copy = pltpu.make_async_copy(src, dst, load_sem.at[len(loads)])
        copy.start()
        loads[name] = copy

    load("x", x_hbm, gx.at[tp])
    barrier = pltpu.get_barrier_semaphore()
    for m in tp_offsets:
        pl.semaphore_signal(
            barrier, inc=1, device_id=peer(tp_to(m), dp), device_id_type=pl.DeviceIdType.MESH
        )
    for to in dp_others:
        pl.semaphore_signal(
            barrier, inc=1, device_id=peer(tp, to), device_id_type=pl.DeviceIdType.MESH
        )
    load("gain", gain_hbm, gain_ref)
    load("ceiling", ceiling_hbm, ceiling_ref)
    load("rescale", rescale_hbm, rescale_ref)
    load("fade", fade_hbm, fade_ref)
    for b in range(blocks):
        for p in range(6):
            load(("w", b, p), weights[p].at[b], wv.at[b, p])
        load(("m", b), memory_hbm.at[b], mem.at[b])
        load(("e", b), exit_hbm.at[b], ev.at[b])

    xs[...] = jnp.zeros_like(xs)
    loads["x"].wait()
    pl.semaphore_wait(barrier, n_tp - 1 + len(dp_others))

    first = []
    for m in tp_offsets:
        first.append(remote(gx.at[tp], gx.at[tp], peer(tp_to(m), dp), gx.at[tp_to(m)]))

    row_at = lax.broadcasted_iota(jnp.int32, (PAD, 1), 0)
    live_col = jnp.zeros((PAD, 1), F32)
    for s in range(seqs):
        for t in range(steps):
            live_col = jnp.where(
                row_at == t * seqs + s, jnp.where(live_ref[s] > t, 1.0, 0.0), live_col
            )
    live3 = [
        live_col[t * seqs : (t + 1) * seqs].reshape(1, seqs, 1) for t in range(steps)
    ]
    on_row = lax.broadcasted_iota(jnp.int32, (n_dp * PAD, LANES), 1) == (
        lax.broadcasted_iota(jnp.int32, (n_dp * PAD, LANES), 0) % PAD
    )
    kinds = 2 * steps * seqs
    deep = -(-kinds // 16) * 16
    kind_at = lax.broadcasted_iota(jnp.int32, (together * deep, 1), 0) % deep % seqs
    slot_at = lax.broadcasted_iota(jnp.int32, (3 * deep, 1), 0) % deep % seqs
    filler = [jnp.zeros((together, deep - kinds, size), F32)] * (deep > kinds)

    def split_states(b):
        loads[("m", b)].wait()
        for s in range(seqs):
            state = mem[b, s].reshape(heads * size, size)
            high = state.astype(BF16)
            low = (state - high.astype(F32)).astype(BF16)
            s_cat[b, s, :, 0:size] = high
            s_cat[b, s, :, size : 2 * size] = high
            s_cat[b, s, :, 2 * size : 3 * size] = low

    for name in ("gain", "ceiling", "rescale", "fade"):
        loads[name].wait()
    split_states(0)
    for p in range(6):
        loads[("w", 0, p)].wait()
    for copy in first:
        copy.wait_recv()
    for i in range(n_tp):
        whole = gx[i].astype(F32)
        for g in range(per_tp):
            xs[(i * per_tp + g) * PAD : (i * per_tp + g) * PAD + rows, :] = slot_major(
                whole[g * rows : (g + 1) * rows]
            )

    for b in range(blocks):
        older = len(outgoing)

        def settle(c):
            for copy in shared[c]:
                copy.wait_recv()
            lanes = slice(c * cut_feats, (c + 1) * cut_feats)
            for i in range(n_dp // dests):
                total = precv[b - 1, 0, c, i].astype(F32)
                for k in range(1, n_tp - 1):
                    total = total + precv[b - 1, k, c, i].astype(F32)
                total, extra = unpack(total, dests * cut_tiles, rows, 0)
                for k in range(dests):
                    at = (i * dests + k) * PAD
                    mine = total[:, k * cut_feats : (k + 1) * cut_feats]
                    mine = mine + part[c][at : at + PAD]
                    xs[at : at + PAD, lanes] = (
                        (xs[at : at + PAD, lanes] + mine).astype(BF16).astype(F32)
                    )

        if b > 0:
            for c in range(cuts):
                settle(c)
        x_now = xs[...]
        gained = (x_now * gain_ref[b : b + 1, :].astype(F32)).astype(BF16)

        def project(slots, g):
            return jnp.concatenate(
                [
                    jnp.dot(
                        gained,
                        wv[b, p, :, g * wide : (g + 1) * wide],
                        preferred_element_type=F32,
                    )
                    for p in slots
                ],
                axis=1,
            )

        scattered = {}

        def scatter(i, values):
            tiles = piece_shape(pieces[i], per_proj)
            for j in range(n_dp):
                block = values[j * PAD : (j + 1) * PAD]
                cut = [block[:, t * LANES : (t + 1) * LANES] for t in range(tiles)]
                zsend[i][b, j] = pack(cut, rows, []).astype(BF16)
            scattered[i] = spread(lambda to: zsend[i].at[b, to], lambda at: zrecv[i].at[b, at])

        halves = [
            sorted(k for g_at, whole, kinds in pieces if g_at == g and not whole for k in kinds)
            for g in range(groups)
        ]
        pairs, own = [], []

        def give(g, values):
            width = len(halves[g]) * wide
            dsend[b, g, :, 0:width] = values.astype(BF16)
            pairs.append(
                remote(
                    dsend.at[b, g, :, pl.ds(0, width)],
                    drecv.at[b, g, :, pl.ds(0, width)],
                    peer(tp, sibling),
                )
            )

        def theirs(g):
            return [3 * other + k for k in halves[g]]

        reduced = [g for g in range(groups) if halves[g]]
        give(0, project(theirs(0), 0))
        squares = jnp.sum(x_now * x_now, axis=1, keepdims=True)
        lined = jnp.where(on_row, squares, 0.0).reshape(n_dp, PAD, LANES)
        lined = jnp.sum(lined, axis=1)
        lined_high = lined.astype(BF16).astype(F32)
        lined_low = lined - lined_high
        for j in range(n_dp):
            qsend[b, j] = jnp.where(
                row_at == 0, lined_high[j : j + 1], lined_low[j : j + 1]
            ).astype(BF16)
        noted = spread(lambda to: qsend.at[b, to], lambda at: qrecv.at[b, at])
        for i, (g, whole, kinds) in enumerate(pieces):
            if whole:
                scatter(i, project([3 * h + k for h in range(2) for k in kinds], g))
        for g in reduced[1:]:
            give(g, project(theirs(g), g))
        for n, g in enumerate(reduced):
            own.append(project([3 * core + k for k in halves[g]], g))
            pairs[n].wait_recv()
            both = own[n] + drecv[b, g, :, 0 : len(halves[g]) * wide].astype(F32)
            for i, (g_at, whole, kinds) in enumerate(pieces):
                if g_at == g and not whole:
                    at = halves[g].index(kinds[0]) * wide
                    scatter(i, both[:, at : at + len(kinds) * wide])
        for i in range(len(pieces)):
            zrecv[i][b, dp] = zsend[i][b, dp]
        qrecv[b, dp] = qsend[b, dp]
        if b > 0:
            split_states(b)
        flush(older)
        spent = len(outgoing)
        fade_b = slot_major(fade_ref[:, b, :])
        fade_b = jnp.concatenate([fade_b, jnp.zeros((PAD - rows, heads), F32)], axis=0)
        row_scale = None

        gathered, later = [], []
        for g in range(groups):
            values = {}

            def arrive(slot):
                nonlocal row_scale
                i = next(
                    i
                    for i, (g_at, whole, kinds) in enumerate(pieces)
                    if g_at == g and slot % 3 in kinds
                )
                whole, kinds = pieces[i][1:]
                tiles = piece_shape(pieces[i], per_proj)
                if row_scale is None:
                    for way in reversed(noted):
                        way.wait_recv()
                    line = qrecv[b, 0].astype(F32)
                    for at in range(1, n_dp):
                        line = line + qrecv[b, at].astype(F32)
                    line = line[0:1] + line[1:2]
                    total_squares = jnp.sum(
                        jnp.where(on_row[0:PAD], line, 0.0), axis=1, keepdims=True
                    )
                    row_scale = lax.rsqrt(total_squares / (feats * n_dp) + NORM_EPS)
                for way in reversed(scattered[i]):
                    way.wait_recv()
                sums = []
                for h in range(2):
                    total = zrecv[i][b, h].astype(F32)
                    for at in range(1, nz):
                        total = total + zrecv[i][b, 2 * at + h].astype(F32)
                    sums.append(total)
                named = [[3 * h + k for k in kinds] for h in range(2)]
                if whole:
                    sums, named = [sums[0] + sums[1]], [named[0] + named[1]]
                for total, names in zip(sums, named):
                    total, extra = unpack(total, tiles, rows, 0)
                    for n, name in enumerate(names):
                        values[name] = total[:, n * wide : (n + 1) * wide] * row_scale

            def flat(slot):
                if slot not in values:
                    arrive(slot)
                return values[slot]

            def by_head(slot):
                rows_now = flat(slot)
                return jnp.stack(
                    [rows_now[:, h * size : (h + 1) * size] for h in range(together)]
                )

            def slots(values):
                return [values[:, t * seqs : (t + 1) * seqs, :] for t in range(steps)]

            key3, fade3 = by_head(0), by_head(3)
            ceiling = ceiling_ref[b : b + 1, g * wide : (g + 1) * wide]
            decay3 = jnp.stack(
                [
                    jnp.exp(
                        fade_b[:, g * together + h : g * together + h + 1]
                        - ceiling[:, h * size : (h + 1) * size] * jax.nn.sigmoid(fade3[h])
                    )
                    for h in range(together)
                ]
            )
            unit3 = key3 * lax.rsqrt(jnp.sum(key3 * key3, axis=2, keepdims=True) + KEY_EPS)
            key, decay, unit = slots(key3), slots(decay3), slots(unit3)
            read = slots(by_head(1))

            wanted = []
            before = None
            for t in range(steps):
                wanted.append(unit[t] if before is None else before * unit[t])
                before = decay[t] if before is None else before * decay[t]
                wanted.append(before * read[t])
            wanted = jnp.concatenate(wanted + filler, axis=1).reshape(together * deep, size)
            wanted_high = wanted.astype(BF16).astype(F32)
            lhs = jnp.concatenate(
                [wanted_high, wanted - wanted_high, wanted_high], axis=1
            ).astype(BF16)
            found = None
            for s in range(seqs):
                product = lax.dot_general(
                    lhs,
                    s_cat[b, s, g * wide : (g + 1) * wide, :],
                    (((1,), (1,)), ((), ())),
                    preferred_element_type=F32,
                )
                found = product if found is None else jnp.where(kind_at == s, product, found)
            found3 = jnp.stack(
                [
                    found[h * deep : (h + 1) * deep, h * size : (h + 1) * size]
                    for h in range(together)
                ]
            )
            pull = slots(unit3 * jax.nn.sigmoid(by_head(4)))
            base = [found3[:, i * seqs : (i + 1) * seqs, :] for i in range(2 * steps)]

            def dot3(a, c):
                return jnp.sum(a * c, axis=2, keepdims=True)

            def weigh(count, vector):
                pairs = []
                for i in range(count - 1, -1, -1):
                    pairs.append((i, dot3(pull[i], vector), dot3(key[i], vector)))
                    if i:
                        vector = decay[i] * vector
                return pairs

            weighed = [(weigh(t, unit[t]), weigh(t + 1, read[t])) for t in range(steps)]
            value = slots(by_head(2))
            taken, readouts = [], []

            def state_times(start, pairs):
                for i, pulled, keyed in pairs:
                    start = start - pulled * taken[i] + keyed * value[i]
                return start

            for t in range(steps):
                taken.append(state_times(base[2 * t], weighed[t][0]))
                readouts.append(state_times(base[2 * t + 1], weighed[t][1]))
            readout = jnp.concatenate(readouts, axis=1)
            centered = readout - jnp.mean(readout, axis=2, keepdims=True)
            normed = centered * lax.rsqrt(
                jnp.mean(centered * centered, axis=2, keepdims=True) + GROUP_EPS
            )
            normed_rows = jnp.concatenate([normed[h] for h in range(together)], axis=1)
            gate = jax.nn.sigmoid(flat(5)[0:rows])
            rescale = rescale_ref[b : b + 1, g * wide : (g + 1) * wide]
            mixed = normed_rows * rescale * gate * live_col[0:rows]
            mixed = jnp.concatenate([mixed, jnp.zeros((PAD - rows, wide), F32)], axis=0)
            mbuf[b, g, dp] = mixed.astype(BF16)
            gathered.append(
                spread(lambda to: mbuf.at[b, g, dp], lambda at: mbuf.at[b, g, at])
            )
            later.append((taken, value, pull, key, decay))

        @pl.when(core >= 0)
        def _():
            for g in range(groups):
                taken, value, pull, key, decay = later[g]
                left, right = [], []
                after = None
                for t in range(steps - 1, -1, -1):
                    left += [-taken[t] * live3[t], value[t] * live3[t]]
                    right += [pull[t] if after is None else pull[t] * after]
                    right += [key[t] if after is None else key[t] * after]
                    kept = jnp.where(live3[t] > 0.0, decay[t], 1.0)
                    after = kept if after is None else after * kept
                left = jnp.concatenate(left + filler, axis=1)
                right = jnp.concatenate(right + filler, axis=1)
                left_high = left.astype(BF16).astype(F32)
                right_high = right.astype(BF16).astype(F32)
                left = jnp.concatenate([left_high, left - left_high, left_high], axis=1).astype(BF16)
                right = jnp.concatenate([right_high, right_high, right - right_high], axis=1)
                for s in range(seqs):
                    for h in range(together):
                        at = g * together + h
                        mine = jnp.where(slot_at == s, right[h], 0.0).astype(BF16)
                        state_ref[b, s, at] = mem[b, s, at] * after[h, s : s + 1, :] + lax.dot_general(
                            left[h], mine, (((0,), (0,)), ((), ())), preferred_element_type=F32
                        )

        flush(spent)
        loads[("e", b)].wait()
        if b < blocks - 1:
            for p in range(6):
                loads[("w", b + 1, p)].wait()
        every = None
        for g in range(groups):
            for way in reversed(gathered[g]):
                way.wait_recv()
            mixed_rows = mbuf[b, g].astype(F32).reshape(n_dp * PAD, wide).astype(BF16)
            product = jnp.dot(
                mixed_rows, ev[b, g * wide : (g + 1) * wide], preferred_element_type=F32
            )
            every = product if every is None else every + product
        part, shared = [], []
        for c in range(cuts):
            value = every[:, c * cut_feats : (c + 1) * cut_feats]
            part.append(value)
            for i in range(n_dp // dests):
                cut = [
                    value[at * PAD : (at + 1) * PAD, t * LANES : (t + 1) * LANES]
                    for at in range(i * dests, (i + 1) * dests)
                    for t in range(cut_tiles)
                ]
                psend[b, c, i] = pack(cut, rows, []).astype(BF16)
            if b < blocks - 1:
                shared.append(
                    [
                        remote(psend.at[b, c], precv.at[b, k, c], peer(tp_to(m), dp))
                        for k, m in enumerate(tp_offsets)
                    ]
                )
    b = blocks - 1
    last = []
    places = per_tp // dests
    for k, m in enumerate(tp_offsets):
        to = tp_to(m)
        last.append(
            remote(
                psend.at[b, :, pl.ds(to * places, places)],
                precv.at[b, k, :, pl.ds(0, places)],
                peer(to, dp),
            )
        )
    pown[...] = xs[...] + jnp.concatenate(part, axis=1)
    flush(len(outgoing) - len(last))
    for copy in last:
        copy.wait_recv()
    finished = []
    for i in range(places):
        found = []
        for c in range(cuts):
            total = precv[b, 0, c, i].astype(F32)
            for k in range(1, n_tp - 1):
                total = total + precv[b, k, c, i].astype(F32)
            found.append(unpack(total, dests * cut_tiles, rows, 0)[0])
        for k in range(dests):
            at = pl.multiple_of((tp * per_tp + i * dests + k) * PAD, PAD)
            total = jnp.concatenate(
                [f[:, k * cut_feats : (k + 1) * cut_feats] for f in found], axis=1
            )
            finished.append(sequence_major((pown[pl.ds(at, PAD), :] + total)[0:rows]))
    out_ref[...] = jnp.concatenate(finished, axis=0).astype(BF16)

    flush(len(outgoing))


def store_kernel(out_vmem, state_vmem, out_hbm, state_hbm, sem):
    blocks, seqs = state_vmem.shape[0:2]
    copies = [
        pltpu.make_async_copy(
            state_vmem.at[b, i], state_hbm.at[b, i], sem.at[b * seqs + i]
        )
        for b in range(blocks)
        for i in range(seqs)
    ]
    copies.append(pltpu.make_async_copy(out_vmem, out_hbm, sem.at[blocks * seqs]))
    for copy in copies:
        copy.start()
    for copy in copies:
        copy.wait()


def solution(mesh):
    n_tp, n_dp = mesh.shape["tp"], mesh.shape["dp"]

    def shards(
        hidden,
        live,
        gain,
        w0,
        w1,
        w2,
        w3,
        w4,
        w5,
        ceiling,
        rescale,
        exit_w,
        memories,
        fade,
    ):
        blocks, feats, chans = w0.shape
        seqs, heads, size = memories.shape[1], memories.shape[2], memories.shape[3]
        rows = fade.shape[1]
        together = max(d for d in range(1, heads + 1) if heads % d == 0 and d * size <= WIDEST)
        groups, wide = heads // together, together * size
        pieces = pieces_of(groups)
        shapes = [piece_shape(piece, wide // LANES) for piece in pieces]
        packed = [LANES * packing(tiles, rows, 0)[0] for tiles in shapes]
        cuts = 1
        dests = 2 if n_dp // n_tp % 2 == 0 else 1
        sent = LANES * packing(dests * (feats // cuts // LANES), rows, 0)[0]
        copies = (n_tp - 1) * (1 + blocks * cuts) + blocks * groups
        copies += blocks * (1 + groups + len(pieces)) * n_dp
        outputs = 4 * blocks * seqs * heads * size * (-(-size // LANES) * LANES)
        outputs += 4 * hidden.shape[0] * hidden.shape[1]
        vmem = pl.BlockSpec(memory_space=pltpu.VMEM)
        smem = pl.BlockSpec(memory_space=pltpu.SMEM)
        hbm = pl.BlockSpec(memory_space=pl.ANY)
        placed = pl.pallas_call(
            functools.partial(kernel, n_tp, n_dp),
            out_shape=(
                pltpu.VMEM(hidden.shape, hidden.dtype),
                pltpu.VMEM(memories.shape, memories.dtype),
            ),
            in_specs=[hbm, smem] + [hbm] * 12,
            out_specs=(vmem, vmem),
            scratch_shapes=[
                pltpu.VMEM((blocks, 6, feats, chans), BF16),
                pltpu.VMEM((blocks, chans, feats), BF16),
                pltpu.VMEM((blocks, seqs, heads, size, size), F32),
                pltpu.VMEM((n_tp,) + hidden.shape, BF16),
                pltpu.VMEM((n_dp * PAD, feats), F32),
                pltpu.VMEM((n_dp * PAD, feats), F32),
                pltpu.VMEM((blocks, groups, n_dp * PAD, 3 * wide), BF16),
                pltpu.VMEM((blocks, groups, n_dp * PAD, 3 * wide), BF16),
                pltpu.VMEM((blocks, groups, n_dp, PAD, wide), BF16),
                pltpu.VMEM((blocks, cuts, n_dp // dests, PAD, sent), BF16),
                pltpu.VMEM((blocks, n_tp - 1, cuts, n_dp // dests, PAD, sent), BF16),
                pltpu.VMEM((blocks, n_dp, PAD, LANES), BF16),
                pltpu.VMEM((blocks, n_dp, PAD, LANES), BF16),
                pltpu.VMEM(gain.shape, BF16),
                pltpu.VMEM(ceiling.shape, F32),
                pltpu.VMEM(rescale.shape, F32),
                pltpu.VMEM((rows, blocks, fade.shape[2]), F32),
                pltpu.VMEM((blocks, seqs, heads * size, 3 * size), BF16),
                pltpu.SemaphoreType.DMA((blocks * 8 + 5,)),
                pltpu.SemaphoreType.DMA((copies,)),
                pltpu.SemaphoreType.DMA((copies,)),
            ]
            + [
                pltpu.VMEM((blocks, n_dp, PAD, width), BF16)
                for width in packed
                for _ in range(2)
            ],
            compiler_params=pltpu.CompilerParams(
                collective_id=0, has_side_effects=True, vmem_limit_bytes=VMEM_BYTES - outputs
            ),
        )(hidden, live, gain, w0, w1, w2, w3, w4, w5, ceiling, rescale, exit_w, memories, fade.transpose(1, 0, 2))
        return pl.pallas_call(
            store_kernel,
            out_shape=(
                jax.ShapeDtypeStruct(hidden.shape, hidden.dtype),
                jax.ShapeDtypeStruct(memories.shape, memories.dtype),
            ),
            in_specs=[vmem, vmem],
            out_specs=(hbm, hbm),
            scratch_shapes=[pltpu.SemaphoreType.DMA((blocks * seqs + 1,))],
            compiler_params=pltpu.CompilerParams(vmem_limit_bytes=1048576),
        )(*placed)

    in_specs = (
        P("tp", "dp"),
        P("dp"),
        P(None, "dp"),
        P(None, "dp", "tp"),
        P(None, "dp", "tp"),
        P(None, "dp", "tp"),
        P(None, "dp", "tp"),
        P(None, "dp", "tp"),
        P(None, "dp", "tp"),
        P(None, "tp"),
        P(None, "tp"),
        P(None, "tp", "dp"),
        P(None, "dp", "tp", None, None),
        P(None, "dp", "tp"),
    )
    out_specs = (P("tp", "dp"), P(None, "dp", "tp", None, None))
    return jax.shard_map(shards, mesh=mesh, in_specs=in_specs, out_specs=out_specs, check_vma=False)
```
